256 devices in a mesh: sp: 64 (over z, y, core), tp: 4 (over x).
Axes of the slice: x: 4, y: 4, z: 8, core: 2. Of those that a mesh axis runs over, the one named last changes fastest.
Arguments:
- query: bfloat16 [16384, 1024], P('sp', 'tp'), may hold values from -12 to 12
- key_rows: bfloat16 [16384, 512], P('sp', 'tp'), may hold values from -8 to 8
- value_rows: bfloat16 [16384, 512], P('sp', 'tp'), may hold values from -16 to 16
- stream: bfloat16 [16384, 2048], P(('sp', 'tp')), may hold values from -6 to 6
- out_weight: bfloat16 [1024, 2048], P('tp'), may hold values from -0.1875 to 0.1875
- norm_gain: float32 [2048], replicated, may hold values from 0.1 to 1.9
- route_ids: int32 [16384, 4], P(('sp', 'tp')), may hold values from 0 to 63, all different within a row; in each aligned block of 64 rows (0 to 63, 64 to 127, ...) at most 8 rows name the same one
- route_weights: float32 [16384, 4], P(('sp', 'tp')), may hold values from 0.1 to 1
- expert_gate: bfloat16 [64, 2048, 384], P('sp'), may hold values from -0.125 to 0.125
- expert_up: bfloat16 [64, 2048, 384], P('sp'), may hold values from -0.125 to 0.125
- expert_down: bfloat16 [64, 384, 2048], P('sp'), may hold values from -0.3125 to 0.3125
- shared_gate: bfloat16 [2048, 384], replicated, may hold values from -0.125 to 0.125
- shared_up: bfloat16 [2048, 384], replicated, may hold values from -0.125 to 0.125
- shared_down: bfloat16 [384, 2048], replicated, may hold values from -0.3125 to 0.3125
Outputs:
- result: bfloat16 [16384, 2048], P(('sp', 'tp'))
The draws below stay inside these ranges and needn't reach their ends.
Inputs may be any that keep to these rules, and one draw needn't show every extreme that they name: `route_ids`: each row names 4 different experts. Within the rows of one device (aligned blocks of 64 rows) no expert is named more than 8 times, and in some blocks one expert is named exactly 8 times.
All inputs are finite; a program needn't handle non-finite values.
Results may differ from the reference program's by a relative error of at most 0.007.
Values may be sent and summed in bfloat16 or wider, within the bound.
No kernel may reach another device: no remote copies, remote signals or barrier semaphores. Data moves between devices by JAX's collectives and lax.ppermute only.
A program may use at most 128 MiB of HBM per device.

```python
import math
import jax
import jax.numpy as jnp
import numpy as np
from jax import lax

D = 2048
HEADS = 8
KV_HEADS = 4
HD = 128
FE = 384
SH = 384
TOP_K = 4
KB = 128
TOK_DEV = 256
TOKEN_SLOTS = 16384
EXPERTS = 64
ROWS = 64
CAP = 8
NBLK = 128


anchor_count = 4


tag_amplitude = 12.0


def common_direction(key):
    raw = jax.random.normal(jax.random.fold_in(key, 101), (KV_HEADS, HD), jnp.float32)
    return raw / jnp.sqrt(jnp.sum(raw * raw, axis=1, keepdims=True)) * HD ** 0.25


def anchor_tags(key):
    direction = common_direction(key)
    unit_dir = direction / jnp.sqrt(jnp.sum(direction * direction, axis=1, keepdims=True))
    partition_count = TOKEN_SLOTS // TOK_DEV
    raw = jax.random.normal(jax.random.fold_in(key, 201), (KV_HEADS, partition_count, anchor_count, HD), jnp.float32)
    along = jnp.sum(raw * unit_dir[:, None, None, :], axis=3, keepdims=True)
    raw = raw - along * unit_dir[:, None, None, :]
    return raw / jnp.sqrt(jnp.sum(raw * raw, axis=3, keepdims=True))


def anchor_offsets(key):
    partition_count = TOKEN_SLOTS // TOK_DEV
    return jax.random.randint(jax.random.fold_in(key, 202), (KV_HEADS, partition_count, anchor_count), 0, TOK_DEV)


def draw_query(key, part):
    direction = common_direction(key)
    fast_share = 0.5
    noise = 0.5 * jax.random.normal(jax.random.fold_in(key, 1), (TOKEN_SLOTS, HEADS, HD), jnp.float32)
    fast = jax.random.uniform(jax.random.fold_in(key, 2), (HEADS,), jnp.float32) < fast_share
    level = jnp.where(fast, -math.log(40.0), -math.log(float(TOKEN_SLOTS))) - 0.4
    head_direction = jnp.repeat(direction, HEADS // KV_HEADS, axis=0)
    shard_of = jnp.arange(TOKEN_SLOTS, dtype=jnp.int32) // TOK_DEV
    target_shard = jax.random.randint(jax.random.fold_in(key, 203), (TOKEN_SLOTS, HEADS), 0, jnp.maximum(shard_of, 1)[:, None])
    target_anchor = jax.random.randint(jax.random.fold_in(key, 204), (TOKEN_SLOTS, HEADS), 0, anchor_count)
    kv_index = jnp.arange(HEADS, dtype=jnp.int32) // (HEADS // KV_HEADS)
    tags = anchor_tags(key)
    chosen = tags[kv_index[None, :], target_shard, target_anchor]
    target_score = jax.random.uniform(jax.random.fold_in(key, 205), (TOKEN_SLOTS, HEADS), jnp.float32, 0.0, 3.0)
    strength = (target_score - level[None, :]) * math.sqrt(HD) / tag_amplitude
    strength = jnp.where(shard_of[:, None] > 0, strength, 0.0)
    full = noise + level[None, :, None] * head_direction[None] + strength[:, :, None] * chosen
    return jnp.clip(full, -12.0, 12.0).reshape(TOKEN_SLOTS, HEADS * HD).astype(jnp.bfloat16)


def draw_key_rows(key, part):
    direction = common_direction(key)
    noise = 0.3 * jax.random.normal(jax.random.fold_in(key, 3), (TOKEN_SLOTS, KV_HEADS, HD), jnp.float32)
    partition_count = TOKEN_SLOTS // TOK_DEV
    shift_amount = jax.random.uniform(jax.random.fold_in(key, 4), (partition_count,), jnp.float32, -0.12, 0.12)
    row_scale = 1.0 + jnp.repeat(shift_amount, TOK_DEV)
    breakage_position = jax.random.randint(jax.random.fold_in(key, 5), (6,), 0, TOKEN_SLOTS)
    broken_weight = jnp.any(jnp.arange(TOKEN_SLOTS)[:, None] == breakage_position[None, :], axis=1)
    row_scale = jnp.where(broken_weight, 0.05, row_scale)
    tags = anchor_tags(key)
    shard_start = jnp.arange(partition_count, dtype=jnp.int32) * TOK_DEV
    positions = (shard_start[None, :, None] + anchor_offsets(key)).reshape(-1)
    head_index = jnp.repeat(jnp.arange(KV_HEADS, dtype=jnp.int32), partition_count * anchor_count)
    planted = jnp.zeros((TOKEN_SLOTS, KV_HEADS, HD), jnp.float32).at[positions, head_index].add(tag_amplitude * tags.reshape(-1, HD))
    full = noise + row_scale[:, None, None] * direction[None] + planted
    return jnp.clip(full, -8.0, 8.0).reshape(TOKEN_SLOTS, KV_HEADS * HD).astype(jnp.bfloat16)


def draw_value_rows(key, part):
    partition_count = TOKEN_SLOTS // TOK_DEV
    noise = 2.0 * jax.random.normal(jax.random.fold_in(key, 6), (TOKEN_SLOTS, KV_HEADS * HD), jnp.float32)
    offsets = 0.5 * jax.random.normal(jax.random.fold_in(key, 7), (partition_count, KV_HEADS * HD), jnp.float32)
    full = noise + jnp.repeat(offsets, TOK_DEV, axis=0)
    return jnp.clip(full, -16.0, 16.0).astype(jnp.bfloat16)


def shard_levels(rng, dims, shards, low, largest):
    def one(dim, blocks):
        steps = jax.random.uniform(jax.random.fold_in(jax.random.fold_in(rng, 6), dim), (blocks,), jnp.float32, low / len(shards), largest / len(shards))
        return jnp.repeat(jnp.exp(steps), dims[dim] // blocks).reshape((-1,) + (1,) * (len(dims) - dim - 1))

    factor_of = one(*shards[0])
    for cut in shards[1:]:
        factor_of = factor_of * one(*cut)
    return factor_of


def assign_block(stream_key, own, number, rows, amount, top, most, skew):
    order = jax.random.permutation(stream_key, amount)
    packed, ordinary = portions_of(amount, rows * top, most, skew, True), portions_of(amount, rows * top, most, skew, False)
    places = jnp.arange(amount)

    def named(tallies, turn):
        used = int((tallies > 0).sum())
        fixed = max(1, used // 4)
        shifted = fixed + (places - fixed + turn * (used - fixed)) % max(1, amount - fixed)
        return jnp.zeros((amount,), jnp.int32).at[order[jnp.where(places < fixed, places, shifted)]].set(jnp.asarray(tallies, jnp.int32))

    tallies = jnp.where(number % 4 == 0, named(packed, number // 4), named(ordinary, number - number // 4 - 1))
    mixed = jax.random.permutation(jax.random.fold_in(own, 3), amount)
    donor, sink = mixed[0:amount // 2 * 2:2], mixed[1:amount // 2 * 2:2]
    margin = jnp.minimum(tallies[donor] - 1, most - tallies[sink]) // 2
    margin = jnp.where((donor == order[0]) | (sink == order[0]) | (tallies[sink] == 0), 0, jnp.maximum(margin, 0))
    shifted = jax.random.randint(jax.random.fold_in(own, 4), (amount // 2,), 0, 1 << 20) % (margin + 1)
    tallies = tallies.at[donor].add(-shifted).at[sink].add(shifted)
    members = jnp.searchsorted(jnp.cumsum(tallies), jnp.arange(rows * top), side="right").astype(jnp.int32)
    listing = members.reshape(top, rows).T
    listing = listing[jax.random.permutation(jax.random.fold_in(own, 1), rows)]
    turn = jax.random.randint(jax.random.fold_in(own, 2), (rows, 1), 0, top)
    return jnp.take_along_axis(listing, (jnp.arange(top)[None, :] + turn) % top, axis=1)


def portions_of(number_of, total, limit, skew, full):
    portions = [(1 << 20) // math.isqrt(grade ** skew) + 1 for grade in range(1, number_of + 1)]
    largest = limit if full else min(limit, max(-(-total // number_of), total * portions[0] // sum(portions)))
    least = 1 if total - largest >= number_of - 1 else 0
    holding, surplus = [largest] + [least] * (number_of - 1), total - largest - least * (number_of - 1)
    while surplus > 0:
        free = [i for i in range(1, number_of) if holding[i] < largest] or [i for i in range(1, number_of) if holding[i] < limit]
        pool, budget = sum([portions[i] for i in free]), surplus
        for i in free:
            extra = min(limit - holding[i], max(1, budget * portions[i] // pool), surplus)
            holding[i] = holding[i] + extra
            surplus = surplus - extra
    return np.array(holding)


def centred(rng, shape, spread, reach, pieces=(), kind=jnp.bfloat16):
    values = spread * jax.random.normal(rng, shape, jnp.float32)
    if pieces:
        values = values * shard_levels(rng, shape, pieces, -0.22, 0.18)
    return jnp.clip(values, -reach, reach).astype(kind)


def setup_inputs(seed: int = 0) -> dict:
    key_list = jax.random.split(jax.random.key(seed), 15)
    query = draw_query(jax.random.fold_in(key_list[14], 71), 0)
    key_rows = draw_key_rows(jax.random.fold_in(key_list[14], 71), 0)
    value_rows = draw_value_rows(jax.random.fold_in(key_list[14], 71), 0)
    stream = centred(key_list[3], (TOKEN_SLOTS, D), 1.0, 6.0, ((0, 256),))
    out_weight = centred(key_list[4], (HEADS * HD, D), (HEADS * HD) ** -0.5, 0.1875, ((0, 4),))
    norm_gain = jnp.clip(1.0 + 0.18 * jax.random.normal(key_list[5], (D,), jnp.float32), 0.1, 1.9)
    route_ids_keys = jax.random.split(jax.random.fold_in(key_list[6], 1), TOKEN_SLOTS // ROWS)
    route_ids_turns = jax.random.permutation(jax.random.fold_in(key_list[6], 3), TOKEN_SLOTS // ROWS)
    route_ids = jax.vmap(lambda own, number: assign_block(jax.random.fold_in(key_list[6], 2), own, number, ROWS, EXPERTS, TOP_K, CAP, 2))(route_ids_keys, route_ids_turns).reshape((TOKEN_SLOTS, TOP_K))
    route_weights = jnp.clip(0.1 + 0.9 * jax.random.uniform(key_list[7], (TOKEN_SLOTS, TOP_K), jnp.float32) ** shard_levels(key_list[7], (TOKEN_SLOTS, TOP_K), ((0, 256),), -0.2, 0.2), 0.1, 1.0)
    expert_gate = centred(key_list[8], (EXPERTS, D, FE), D ** -0.5, 0.125, ((0, 64),))
    expert_up = centred(key_list[9], (EXPERTS, D, FE), D ** -0.5, 0.125, ((0, 64),))
    expert_down = centred(key_list[10], (EXPERTS, FE, D), FE ** -0.5, 0.3125, ((0, 64),))
    shared_gate = centred(key_list[11], (D, SH), D ** -0.5, 0.125)
    shared_up = centred(key_list[12], (D, SH), D ** -0.5, 0.125)
    shared_down = centred(key_list[13], (SH, D), SH ** -0.5, 0.3125)
    return {"query": query, "key_rows": key_rows, "value_rows": value_rows, "stream": stream, "out_weight": out_weight, "norm_gain": norm_gain, "route_ids": route_ids, "route_weights": route_weights, "expert_gate": expert_gate, "expert_up": expert_up, "expert_down": expert_down, "shared_gate": shared_gate, "shared_up": shared_up, "shared_down": shared_down}


def soft_plus(values):
    return jnp.maximum(values, 0.0) + jnp.log1p(jnp.exp(-jnp.abs(values)))

def reference(query, key_rows, value_rows, stream, out_weight, norm_gain, route_ids, route_weights, expert_gate, expert_up, expert_down, shared_gate, shared_up, shared_down):
    query_all = query.reshape(TOKEN_SLOTS, HEADS, HD).astype(jnp.float32)
    keys_all = jnp.repeat(key_rows.reshape(TOKEN_SLOTS, KV_HEADS, HD), HEADS // KV_HEADS, axis=1).astype(jnp.float32)
    values_all = jnp.repeat(value_rows.reshape(TOKEN_SLOTS, KV_HEADS, HD), HEADS // KV_HEADS, axis=1).astype(jnp.float32)
    key_pos = jnp.arange(TOKEN_SLOTS, dtype=jnp.int32)

    def attend_block(block_index):
        block_start = (block_index * KB).astype(jnp.int32)
        block_queries = lax.dynamic_slice_in_dim(query_all, block_start, KB, 0)
        logits = jnp.einsum('qhd,shd->hqs', block_queries, keys_all) * (1.0 / math.sqrt(HD))
        query_pos = block_start + jnp.arange(KB, dtype=jnp.int32)
        visible = key_pos[None, :] < query_pos[:, None]
        penalty = soft_plus(logits)
        breaks = jnp.where(visible, -penalty, 0.0)
        between = jnp.cumsum(breaks[:, :, ::-1], axis=2)[:, :, ::-1] - breaks
        weights = jnp.where(visible, jnp.exp(logits - penalty + between), 0.0).astype(jnp.bfloat16)
        mixed = jnp.einsum('hqs,shd->qhd', weights.astype(jnp.float32), values_all)
        return mixed.astype(jnp.bfloat16)
    heads_out = lax.map(attend_block, jnp.arange(NBLK, dtype=jnp.int32)).reshape(TOKEN_SLOTS, HEADS * HD)
    attended = jnp.dot(heads_out, out_weight, preferred_element_type=jnp.float32)
    mid = (stream.astype(jnp.float32) + attended).astype(jnp.bfloat16)
    mid_wide = lax.optimization_barrier(mid).astype(jnp.float32)
    normed = (mid_wide * lax.rsqrt(lax.optimization_barrier(jnp.mean(mid_wide * mid_wide, axis=1, keepdims=True)) + 1e-06) * norm_gain).astype(jnp.bfloat16)
    flat_ids = route_ids.reshape(-1).astype(jnp.int32)
    most_rows = TOKEN_SLOTS // ROWS * CAP
    padded = jnp.concatenate([normed, jnp.zeros((1, D), jnp.bfloat16)], axis=0)

    def one_expert(expert, output_values):
        slot_spots = jnp.nonzero(flat_ids == expert, size=most_rows, fill_value=TOKEN_SLOTS * TOP_K)[0].astype(jnp.int32)
        taken_rows = padded[slot_spots // TOP_K]
        gate_part = jnp.dot(taken_rows, expert_gate[expert], preferred_element_type=jnp.float32)
        up_part = jnp.dot(taken_rows, expert_up[expert], preferred_element_type=jnp.float32)
        hidden = (jax.nn.silu(gate_part) * up_part).astype(jnp.bfloat16)
        produced = jnp.dot(hidden, expert_down[expert], preferred_element_type=jnp.float32).astype(jnp.bfloat16)
        return output_values.at[slot_spots].set(produced)
    output_values = lax.fori_loop(0, EXPERTS, one_expert, jnp.zeros((TOKEN_SLOTS * TOP_K + 1, D), jnp.bfloat16))
    selected_experts = output_values[:TOKEN_SLOTS * TOP_K].astype(jnp.float32).reshape(TOKEN_SLOTS, TOP_K, D)
    routed = lax.optimization_barrier(jnp.sum(selected_experts * route_weights[:, :, None], axis=1))
    shared_hidden = (jax.nn.silu(jnp.dot(normed, shared_gate, preferred_element_type=jnp.float32)) * jnp.dot(normed, shared_up, preferred_element_type=jnp.float32)).astype(jnp.bfloat16)
    shared_out = jnp.dot(shared_hidden, shared_down, preferred_element_type=jnp.float32)
    return (mid_wide + routed + shared_out).astype(jnp.bfloat16)
```

```python
import math

import jax
import jax.numpy as jnp
from jax import lax
from jax.experimental import pallas as pl
from jax.experimental.pallas import tpu as pltpu
from jax.sharding import Mesh
from jax.sharding import PartitionSpec as P

D = 2048
HD = 128
TOP_K = 4
KB = 128
SP = ("sp_0", "sp_1", "sp_2")
SP_TP = ("sp_0", "sp_1", "sp_2", "tp")


BK = 256
SCALE = math.log2(math.e) / math.sqrt(HD)


def attention_kernel(pos_ref, q_ref, kv_ref, o_ref, q2, acc, carry, tri, dbuf, sbuf):
    tok = q_ref.shape[0]
    heads = q_ref.shape[1] // HD
    rows = tok * heads
    for g in range(heads):
        scaled = q_ref[:, g * HD : (g + 1) * HD].astype(jnp.float32) * SCALE
        high = scaled.astype(jnp.bfloat16)
        q2[pl.ds(g * tok, tok), 0:HD] = high
        q2[pl.ds(g * tok, tok), HD : 2 * HD] = (scaled - high.astype(jnp.float32)).astype(
            jnp.bfloat16
        )
    acc[...] = jnp.zeros_like(acc)
    carry[...] = jnp.zeros_like(carry)
    key_at = lax.broadcasted_iota(jnp.int32, (BK, BK), 0)
    tri[...] = (
        (key_at > lax.broadcasted_iota(jnp.int32, (BK, BK), 1))
        .astype(jnp.float32)
        .astype(jnp.bfloat16)
    )
    pos = pos_ref[0]

    def scores(j, slot, diagonal):
        start = pl.multiple_of(j * BK, BK)
        keys = kv_ref[pl.ds(start, BK), 0:HD]
        y = lax.dot_general(
            q2[...],
            jnp.concatenate([keys, keys], axis=1),
            (((1,), (1,)), ((), ())),
            preferred_element_type=jnp.float32,
        )
        penalty = jnp.maximum(y, jnp.log2(1.0 + jnp.exp2(jnp.minimum(y, 126.0))))
        level = y - penalty
        if diagonal:
            query_at = lax.broadcasted_iota(jnp.int32, (rows, BK), 0) % tok
            visible = lax.broadcasted_iota(jnp.int32, (rows, BK), 1) < query_at
            penalty = jnp.where(visible, penalty, 0.0)
            level = jnp.where(visible, level, -1e30)
        dbuf[slot] = level
        sbuf[slot] = penalty.astype(jnp.bfloat16)

    def mix(j, slot):
        start = pl.multiple_of(j * BK, BK)
        values = kv_ref[pl.ds(start, BK), HD : 2 * HD]
        penalty = sbuf[slot]
        after = jnp.dot(penalty, tri[...], preferred_element_type=jnp.float32)
        so_far = carry[...]
        weights = jnp.exp2(dbuf[slot] - after - jnp.concatenate([so_far, so_far], axis=1))
        carry[...] = so_far + jnp.broadcast_to(
            after[:, 0:1] + penalty[:, 0:1].astype(jnp.float32), (rows, HD)
        )
        acc[...] += jnp.dot(
            weights.astype(jnp.bfloat16), values, preferred_element_type=jnp.float32
        )

    def both(j, slot):
        mix(j, slot)
        scores(j - 1, 1 - slot, False)

    scores(pos, 0, True)

    def step(i, _):
        both(pos - 2 * i, 0)
        both(pos - 2 * i - 1, 1)
        return 0

    lax.fori_loop(0, pos // 2, step, 0)

    @pl.when(pos % 2 == 1)
    def _():
        both(1, 0)
        mix(0, 1)

    @pl.when(pos % 2 == 0)
    def _():
        mix(0, 0)

    for g in range(heads):
        o_ref[:, g * HD : (g + 1) * HD] = acc[pl.ds(g * tok, tok), :].astype(o_ref.dtype)


def attention(query, pairs, device_pos):
    tok = query.shape[0]
    rows = tok * (query.shape[1] // HD)
    steps = pairs.shape[0] // BK
    return pl.pallas_call(
        attention_kernel,
        out_shape=jax.ShapeDtypeStruct(query.shape, jnp.bfloat16),
        in_specs=[
            pl.BlockSpec(memory_space=pltpu.SMEM),
            pl.BlockSpec(memory_space=pltpu.VMEM),
            pl.BlockSpec(memory_space=pltpu.VMEM),
        ],
        out_specs=pl.BlockSpec(memory_space=pltpu.VMEM),
        scratch_shapes=[
            pltpu.VMEM((rows, 2 * HD), jnp.bfloat16),
            pltpu.VMEM((rows, HD), jnp.float32),
            pltpu.VMEM((rows, HD), jnp.float32),
            pltpu.VMEM((BK, BK), jnp.bfloat16),
            pltpu.VMEM((2, rows, BK), jnp.float32),
            pltpu.VMEM((2, rows, BK), jnp.bfloat16),
        ],
        compiler_params=pltpu.CompilerParams(vmem_limit_bytes=40 * 2**20),
        cost_estimate=pl.CostEstimate(
            flops=steps * rows * BK * HD * 8, bytes_accessed=pairs.size * 2, transcendentals=0
        ),
        name="stick",
    )(device_pos.reshape(1), query, pairs)


def per_device(
    query,
    key_rows,
    value_rows,
    stream,
    out_weight,
    norm_gain,
    route_ids,
    route_weights,
    expert_gate,
    expert_up,
    expert_down,
    shared_gate,
    shared_up,
    shared_down,
):
    device_pos = lax.axis_index(SP)
    pairs = lax.all_gather(
        jnp.concatenate([key_rows, value_rows], axis=1), SP, axis=0, tiled=True
    )
    heads_out = attention(query, pairs, device_pos)
    own_rows = stream.shape[0]
    token_heads = lax.all_to_all(heads_out, "tp", split_axis=0, concat_axis=1, tiled=True)
    attended = jnp.dot(
        token_heads,
        lax.all_gather(out_weight, "tp", axis=0, tiled=True),
        preferred_element_type=jnp.float32,
    )
    mid = (stream.astype(jnp.float32) + attended).astype(jnp.bfloat16)
    mid_wide = lax.optimization_barrier(mid).astype(jnp.float32)
    normed = (
        mid_wide
        * lax.rsqrt(jnp.mean(mid_wide * mid_wide, axis=1, keepdims=True) + 1e-06)
        * norm_gain
    ).astype(jnp.bfloat16)
    local_experts = expert_gate.shape[0]
    expert_count = lax.axis_size(SP) * local_experts
    capacity = 2 * own_rows * TOP_K // expert_count
    slot_count = expert_count * capacity
    flat_ids = route_ids.reshape(-1)
    membership = (flat_ids[:, None] == jnp.arange(expert_count, dtype=jnp.int32)[None, :]).astype(
        jnp.int32
    )
    before = jnp.cumsum(membership, axis=0) - membership
    slot_rank = jnp.sum(before * membership, axis=1)
    slot_ids = flat_ids * capacity + slot_rank
    placing = jnp.arange(slot_count, dtype=jnp.int32)[:, None] == slot_ids[None, :]
    dispatch = placing.reshape(slot_count, own_rows, TOP_K).any(axis=2).astype(jnp.bfloat16)
    outgoing = jnp.dot(dispatch, normed, preferred_element_type=jnp.float32).astype(jnp.bfloat16)
    outgoing = outgoing.reshape(lax.axis_size(SP), local_experts, capacity, D)
    arrived = lax.all_to_all(outgoing, SP, split_axis=0, concat_axis=0, tiled=True)
    gate_part = jnp.einsum(
        "sepd,edf->sepf", arrived, expert_gate, preferred_element_type=jnp.float32
    )
    up_part = jnp.einsum("sepd,edf->sepf", arrived, expert_up, preferred_element_type=jnp.float32)
    hidden = (jax.nn.silu(gate_part) * up_part).astype(jnp.bfloat16)
    produced = jnp.einsum(
        "sepf,efd->sepd", hidden, expert_down, preferred_element_type=jnp.float32
    ).astype(jnp.bfloat16)
    returned = lax.all_to_all(produced, SP, split_axis=0, concat_axis=0, tiled=True)
    returned = returned.reshape(slot_count, D)
    picking = (slot_ids[:, None] == jnp.arange(slot_count, dtype=jnp.int32)[None, :]).astype(
        jnp.bfloat16
    )
    selected_experts = jnp.dot(picking, returned, preferred_element_type=jnp.float32).reshape(
        own_rows, TOP_K, D
    )
    routed = jnp.sum(selected_experts * route_weights[:, :, None], axis=1)
    shared_hidden = (
        jax.nn.silu(jnp.dot(normed, shared_gate, preferred_element_type=jnp.float32))
        * jnp.dot(normed, shared_up, preferred_element_type=jnp.float32)
    ).astype(jnp.bfloat16)
    shared_out = jnp.dot(shared_hidden, shared_down, preferred_element_type=jnp.float32)
    return (mid_wide + routed + shared_out).astype(jnp.bfloat16)


def solution(mesh):
    split = Mesh(mesh.devices.reshape(8, 4, 2, mesh.shape["tp"]), ("sp_0", "sp_1", "sp_2", "tp"))
    in_specs = (
        P(SP, "tp"),
        P(SP, "tp"),
        P(SP, "tp"),
        P(SP_TP, None),
        P("tp", None),
        P(),
        P(SP_TP, None),
        P(SP_TP, None),
        P(SP, None, None),
        P(SP, None, None),
        P(SP, None, None),
        P(),
        P(),
        P(),
    )
    out_specs = P(SP_TP, None)
    return jax.shard_map(
        per_device, mesh=split, in_specs=in_specs, out_specs=out_specs, check_vma=False
    )
```

```python
import functools
import math

import jax
import jax.numpy as jnp
from jax import lax
from jax.experimental import pallas as pl
from jax.experimental.pallas import tpu as pltpu
from jax.sharding import Mesh
from jax.sharding import PartitionSpec as P


D = 2048
HD = 128
TOP_K = 4
KB = 128
SP = ("sp_0", "sp_1", "sp_2")
SP_TP = ("sp_0", "sp_1", "sp_2", "tp")


BK = 256
SCALE = math.log2(math.e) / math.sqrt(HD)


def shifted(value, axis, step):
    size = lax.axis_size(axis)
    return lax.ppermute(value, axis, [(i, (i + step) % size) for i in range(size)])


def gathered_keys(keys):
    z_size, y_size = lax.axis_size("sp_0"), lax.axis_size("sp_1")
    ring = [keys] + [None] * (y_size - 1)
    down = up = keys
    for k in range(1, y_size // 2 + 1):
        down = ring[k] = shifted(down, "sp_1", 1)
        if k < y_size - k:
            up = ring[y_size - k] = shifted(up, "sp_1", -1)
    planes = [jnp.stack(ring)] + [None] * (z_size - 1)
    half = y_size // 2
    down = up = planes[0]
    for k in range(1, z_size // 2):
        down = planes[k] = shifted(down, "sp_0", 1)
        up = planes[z_size - k] = shifted(up, "sp_0", -1)
    planes[z_size // 2] = jnp.concatenate(
        [shifted(down[:half], "sp_0", 1), shifted(up[half:], "sp_0", -1)]
    )
    others = [shifted(plane, "sp_2", 1) for plane in planes]
    return jnp.concatenate(planes + others).reshape(-1, keys.shape[1])


def attention_kernel(z_size, y_size, pos_ref, q_ref, k_ref, v_ref, o_ref, q2, acc, carry, tri, dbuf, sbuf):
    tok = q_ref.shape[0]
    heads = q_ref.shape[1] // HD
    rows = tok * heads
    for g in range(heads):
        scaled = q_ref[:, g * HD : (g + 1) * HD].astype(jnp.float32) * SCALE
        high = scaled.astype(jnp.bfloat16)
        q2[pl.ds(g * tok, tok), 0:HD] = high
        q2[pl.ds(g * tok, tok), HD : 2 * HD] = (scaled - high.astype(jnp.float32)).astype(
            jnp.bfloat16
        )
    acc[...] = jnp.zeros_like(acc)
    carry[...] = jnp.zeros_like(carry)
    key_at = lax.broadcasted_iota(jnp.int32, (BK, BK), 0)
    tri[...] = (
        (key_at > lax.broadcasted_iota(jnp.int32, (BK, BK), 1))
        .astype(jnp.float32)
        .astype(jnp.bfloat16)
    )
    pos = pos_ref[0]

    def scores(j, slot, diagonal):
        core = (pos + j) % 2
        row = (pos // 2 + y_size - (j // 2) % y_size) % y_size
        plane = pos // (2 * y_size) - j // (2 * y_size)
        start = pl.multiple_of(((core * z_size + plane) * y_size + row) * BK, BK)
        keys = k_ref[pl.ds(start, BK), :]
        y = lax.dot_general(
            q2[...],
            jnp.concatenate([keys, keys], axis=1),
            (((1,), (1,)), ((), ())),
            preferred_element_type=jnp.float32,
        )
        penalty = jnp.maximum(y, jnp.log2(1.0 + jnp.exp2(jnp.minimum(y, 126.0))))
        level = y - penalty
        if diagonal:
            query_at = lax.broadcasted_iota(jnp.int32, (rows, BK), 0) % tok
            visible = lax.broadcasted_iota(jnp.int32, (rows, BK), 1) < query_at
            penalty = jnp.where(visible, penalty, 0.0)
            level = jnp.where(visible, level, -1e30)
        dbuf[slot] = level
        sbuf[slot] = penalty.astype(jnp.bfloat16)

    def mix(j, slot):
        start = pl.multiple_of(j * BK, BK)
        values = v_ref[pl.ds(start, BK), :]
        penalty = sbuf[slot]
        after = jnp.dot(penalty, tri[...], preferred_element_type=jnp.float32)
        so_far = carry[...]
        weights = jnp.exp2(dbuf[slot] - after - jnp.concatenate([so_far, so_far], axis=1))
        carry[...] = so_far + jnp.broadcast_to(
            after[:, 0:1] + penalty[:, 0:1].astype(jnp.float32), (rows, HD)
        )
        acc[...] += jnp.dot(
            weights.astype(jnp.bfloat16), values, preferred_element_type=jnp.float32
        )

    def both(j, slot):
        mix(j, slot)
        scores(j - 1, 1 - slot, False)

    scores(pos, 0, True)

    def step(i, _):
        both(pos - 2 * i, 0)
        both(pos - 2 * i - 1, 1)
        return 0

    lax.fori_loop(0, pos // 2, step, 0)

    @pl.when(pos % 2 == 1)
    def _():
        both(1, 0)
        mix(0, 1)

    @pl.when(pos % 2 == 0)
    def _():
        mix(0, 0)

    for g in range(heads):
        o_ref[:, g * HD : (g + 1) * HD] = acc[pl.ds(g * tok, tok), :].astype(o_ref.dtype)


def attention(query, keys, values, device_pos):
    tok = query.shape[0]
    rows = tok * (query.shape[1] // HD)
    steps = values.shape[0] // BK
    return pl.pallas_call(
        functools.partial(attention_kernel, lax.axis_size("sp_0"), lax.axis_size("sp_1")),
        out_shape=jax.ShapeDtypeStruct(query.shape, jnp.bfloat16),
        in_specs=[
            pl.BlockSpec(memory_space=pltpu.SMEM),
            pl.BlockSpec(memory_space=pltpu.VMEM),
            pl.BlockSpec(memory_space=pltpu.VMEM),
            pl.BlockSpec(memory_space=pltpu.VMEM),
        ],
        out_specs=pl.BlockSpec(memory_space=pltpu.VMEM),
        scratch_shapes=[
            pltpu.VMEM((rows, 2 * HD), jnp.bfloat16),
            pltpu.VMEM((rows, HD), jnp.float32),
            pltpu.VMEM((rows, HD), jnp.float32),
            pltpu.VMEM((BK, BK), jnp.bfloat16),
            pltpu.VMEM((2, rows, BK), jnp.float32),
            pltpu.VMEM((2, rows, BK), jnp.bfloat16),
        ],
        compiler_params=pltpu.CompilerParams(vmem_limit_bytes=40 * 2**20),
        cost_estimate=pl.CostEstimate(
            flops=steps * rows * BK * HD * 8, bytes_accessed=values.size * 4, transcendentals=0
        ),
        name="stick",
    )(device_pos.reshape(1), query, keys, values)


def per_device(
    query,
    key_rows,
    value_rows,
    stream,
    out_weight,
    norm_gain,
    route_ids,
    route_weights,
    expert_gate,
    expert_up,
    expert_down,
    shared_gate,
    shared_up,
    shared_down,
):
    device_pos = lax.axis_index(SP)
    values = lax.all_gather(value_rows, SP, axis=0, tiled=True)
    heads_out = attention(query, gathered_keys(key_rows), values, device_pos)
    own_rows = stream.shape[0]
    token_heads = lax.all_to_all(heads_out, "tp", split_axis=0, concat_axis=1, tiled=True)
    attended = jnp.dot(
        token_heads,
        lax.all_gather(out_weight, "tp", axis=0, tiled=True),
        preferred_element_type=jnp.float32,
    )
    mid = (stream.astype(jnp.float32) + attended).astype(jnp.bfloat16)
    mid_wide = lax.optimization_barrier(mid).astype(jnp.float32)
    normed = (
        mid_wide
        * lax.rsqrt(jnp.mean(mid_wide * mid_wide, axis=1, keepdims=True) + 1e-06)
        * norm_gain
    ).astype(jnp.bfloat16)
    local_experts = expert_gate.shape[0]
    expert_count = lax.axis_size(SP) * local_experts
    capacity = 2 * own_rows * TOP_K // expert_count
    slot_count = expert_count * capacity
    flat_ids = route_ids.reshape(-1)
    membership = (flat_ids[:, None] == jnp.arange(expert_count, dtype=jnp.int32)[None, :]).astype(
        jnp.int32
    )
    before = jnp.cumsum(membership, axis=0) - membership
    slot_rank = jnp.sum(before * membership, axis=1)
    slot_ids = flat_ids * capacity + slot_rank
    placing = jnp.arange(slot_count, dtype=jnp.int32)[:, None] == slot_ids[None, :]
    dispatch = placing.reshape(slot_count, own_rows, TOP_K).any(axis=2).astype(jnp.bfloat16)
    outgoing = jnp.dot(dispatch, normed, preferred_element_type=jnp.float32).astype(jnp.bfloat16)
    outgoing = outgoing.reshape(lax.axis_size(SP), local_experts, capacity, D)
    arrived = lax.all_to_all(outgoing, SP, split_axis=0, concat_axis=0, tiled=True)
    gate_part = jnp.einsum(
        "sepd,edf->sepf", arrived, expert_gate, preferred_element_type=jnp.float32
    )
    up_part = jnp.einsum("sepd,edf->sepf", arrived, expert_up, preferred_element_type=jnp.float32)
    hidden = (jax.nn.silu(gate_part) * up_part).astype(jnp.bfloat16)
    produced = jnp.einsum(
        "sepf,efd->sepd", hidden, expert_down, preferred_element_type=jnp.float32
    ).astype(jnp.bfloat16)
    returned = lax.all_to_all(produced, SP, split_axis=0, concat_axis=0, tiled=True)
    returned = returned.reshape(slot_count, D)
    picking = (slot_ids[:, None] == jnp.arange(slot_count, dtype=jnp.int32)[None, :]).astype(
        jnp.bfloat16
    )
    selected_experts = jnp.dot(picking, returned, preferred_element_type=jnp.float32).reshape(
        own_rows, TOP_K, D
    )
    routed = jnp.sum(selected_experts * route_weights[:, :, None], axis=1)
    shared_hidden = (
        jax.nn.silu(jnp.dot(normed, shared_gate, preferred_element_type=jnp.float32))
        * jnp.dot(normed, shared_up, preferred_element_type=jnp.float32)
    ).astype(jnp.bfloat16)
    shared_out = jnp.dot(shared_hidden, shared_down, preferred_element_type=jnp.float32)
    return (mid_wide + routed + shared_out).astype(jnp.bfloat16)


def solution(mesh):
    split = Mesh(mesh.devices.reshape(8, 4, 2, mesh.shape["tp"]), ("sp_0", "sp_1", "sp_2", "tp"))
    in_specs = (
        P(SP, "tp"),
        P(SP, "tp"),
        P(SP, "tp"),
        P(SP_TP, None),
        P("tp", None),
        P(),
        P(SP_TP, None),
        P(SP_TP, None),
        P(SP, None, None),
        P(SP, None, None),
        P(SP, None, None),
        P(),
        P(),
        P(),
    )
    out_specs = P(SP_TP, None)
    return jax.shard_map(
        per_device, mesh=split, in_specs=in_specs, out_specs=out_specs, check_vma=False
    )
```

```python
import functools
import math

import jax
import jax.numpy as jnp
from jax import lax
from jax.experimental import pallas as pl
from jax.experimental.pallas import tpu as pltpu
from jax.sharding import Mesh
from jax.sharding import PartitionSpec as P


D = 2048
HD = 128
TOP_K = 4
KB = 128
SP = ("sp_0", "sp_1", "sp_2")
SP_TP = ("sp_0", "sp_1", "sp_2", "tp")


BK = 256
SCALE = math.log2(math.e) / math.sqrt(HD)


def shifted(value, axis, step):
    size = lax.axis_size(axis)
    return lax.ppermute(value, axis, [(i, (i + step) % size) for i in range(size)])


def counter_shifted(value):
    size = lax.axis_size("sp_0")
    pairs = [(2 * i, 2 * ((i + 1) % size)) for i in range(size)]
    pairs += [(2 * i + 1, 2 * ((i - 1) % size) + 1) for i in range(size)]
    return lax.ppermute(value, ("sp_0", "sp_2"), pairs)


def call(kernel, outs, args, scratch=(), flops=0, name=None):
    return pl.pallas_call(
        kernel,
        out_shape=[jax.ShapeDtypeStruct(*out) for out in outs],
        in_specs=[pl.BlockSpec(memory_space=pltpu.SMEM)]
        + [pl.BlockSpec(memory_space=pltpu.VMEM)] * (len(args) - 1),
        out_specs=[pl.BlockSpec(memory_space=pltpu.VMEM)] * len(outs),
        scratch_shapes=list(scratch),
        compiler_params=pltpu.CompilerParams(vmem_limit_bytes=24 * 2**20),
        cost_estimate=pl.CostEstimate(flops=flops, bytes_accessed=2**20, transcendentals=0),
        name=name,
    )(*args)


def assemble_kernel(y_size, at_ref, own_ref, other_ref, plane_ref):
    row, core = at_ref[1], at_ref[2]
    for k in range(y_size):
        place = 2 * ((row + y_size - k) % y_size)
        plane_ref[place + core] = own_ref[k]
        plane_ref[place + 1 - core] = other_ref[k]


def block_steps(q_ref, plane_ref, acc, carry, tri, level_buf, penalty_buf, first_row, tok):
    rows = acc.shape[0]

    def scores(j, slot, diagonal=False):
        keys = plane_ref[j, :, 0:HD]
        y = lax.dot_general(
            q_ref[pl.ds(first_row, rows), :],
            jnp.concatenate([keys, keys], axis=1),
            (((1,), (1,)), ((), ())),
            preferred_element_type=jnp.float32,
        )
        penalty = jnp.maximum(y, jnp.log2(1.0 + jnp.exp2(jnp.minimum(y, 126.0))))
        level = y - penalty
        if diagonal:
            query_at = lax.broadcasted_iota(jnp.int32, (rows, BK), 0) % tok
            visible = lax.broadcasted_iota(jnp.int32, (rows, BK), 1) < query_at
            penalty = jnp.where(visible, penalty, 0.0)
            level = jnp.where(visible, level, -1e30)
        level_buf[slot] = level
        penalty_buf[slot] = penalty.astype(jnp.bfloat16)

    def mix(j, slot):
        penalty = penalty_buf[slot]
        after = jnp.dot(penalty, tri[...], preferred_element_type=jnp.float32)
        so_far = carry[...]
        weights = jnp.exp2(level_buf[slot] - after - jnp.concatenate([so_far, so_far], axis=1))
        carry[...] = so_far + jnp.broadcast_to(
            after[:, 0:1] + penalty[:, 0:1].astype(jnp.float32), (rows, HD)
        )
        acc[...] += jnp.dot(
            weights.astype(jnp.bfloat16),
            plane_ref[j, :, HD : 2 * HD],
            preferred_element_type=jnp.float32,
        )

    def both(j, slot):
        mix(j, slot)
        scores(j - 1, 1 - slot)

    return scores, mix, both


def clear(acc, carry, tri):
    acc[...] = jnp.zeros_like(acc)
    carry[...] = jnp.zeros_like(carry)
    key_at = lax.broadcasted_iota(jnp.int32, (BK, BK), 0)
    later = key_at > lax.broadcasted_iota(jnp.int32, (BK, BK), 1)
    tri[...] = later.astype(jnp.float32).astype(jnp.bfloat16)


def own_plane_kernel(
    at_ref, own_ref, other_ref, plane_ref, q_ref, acc, carry, tri, level_buf, penalty_buf
):
    tok = own_ref.shape[0]
    heads = own_ref.shape[1] // HD
    rows = tok * heads
    core = at_ref[2]
    for place, ref in ((core, own_ref), (1 - core, other_ref)):
        for g in range(heads):
            scaled = ref[:, g * HD : (g + 1) * HD].astype(jnp.float32) * SCALE
            high = scaled.astype(jnp.bfloat16)
            target = pl.ds(pl.multiple_of(place * rows + g * tok, tok), tok)
            q_ref[target, 0:HD] = high
            q_ref[target, HD : 2 * HD] = (scaled - high.astype(jnp.float32)).astype(jnp.bfloat16)
    clear(acc, carry, tri)
    first_row = pl.multiple_of(core * rows, rows)
    scores, mix, both = block_steps(
        q_ref, plane_ref, acc, carry, tri, level_buf, penalty_buf, first_row, tok
    )
    pos = 2 * at_ref[1] + core
    scores(pos, 0, diagonal=True)

    def step(i, _):
        both(pos - 2 * i, 0)
        both(pos - 2 * i - 1, 1)
        return 0

    lax.fori_loop(0, pos // 2, step, 0)

    @pl.when(pos % 2 == 1)
    def _():
        both(1, 0)
        mix(0, 1)

    @pl.when(pos % 2 == 0)
    def _():
        mix(0, 0)


def plane_kernel(
    distance, z_size, tok, last, at_ref, q_ref, plane_ref, acc_in, total_in, acc_out, total_out,
    acc, carry, tri, level_buf, penalty_buf
):
    rows = acc.shape[0]
    core = at_ref[2]
    below = jnp.where(core == 0, distance, z_size - distance)
    shards = plane_ref.shape[0]

    def part(h, _):
        first_row = pl.multiple_of(h * rows, rows)
        here = pl.ds(first_row, rows)
        clear(acc, carry, tri)

        @pl.when(below <= at_ref[0])
        def _():
            scores, mix, both = block_steps(
                q_ref, plane_ref, acc, carry, tri, level_buf, penalty_buf, first_row, tok
            )
            scores(shards - 1, 0)

            def step(i, _):
                both(shards - 1 - 2 * i, 0)
                both(shards - 2 - 2 * i, 1)
                return 0

            lax.fori_loop(0, shards // 2 - 1, step, 0)
            both(1, 0)
            mix(0, 1)

        old, old_total = acc_in[here, :], total_in[here, :]
        new, new_total = acc[...], carry[...]
        upward = core == 0
        result = old * jnp.exp2(jnp.where(upward, 0.0, -new_total))
        result = result + new * jnp.exp2(jnp.where(upward, -old_total, 0.0))
        if last:
            place = jnp.where(h == core, 0, 1)
            acc_out[place] = result
            total_out[place] = old_total + new_total
        else:
            acc_out[here, :] = result
            total_out[here, :] = old_total + new_total
        return 0

    lax.fori_loop(0, 2, part, 0)


def merge_kernel(at_ref, own_ref, own_total, acc_ref, total_ref, theirs, their_total, out_ref):
    upward = at_ref[2] == 0
    tok = out_ref.shape[0]
    mine, other = acc_ref[0], theirs[...]
    newer_total = jnp.where(upward, total_ref[0], their_total[...])
    newer, older = jnp.where(upward, mine, other), jnp.where(upward, other, mine)
    mixed = own_ref[...] + jnp.exp2(-own_total[...]) * (newer + jnp.exp2(-newer_total) * older)
    for g in range(out_ref.shape[1] // HD):
        out_ref[:, g * HD : (g + 1) * HD] = mixed[g * tok : (g + 1) * tok].astype(out_ref.dtype)


def attention(query, keys, values):
    z_size, y_size = lax.axis_size("sp_0"), lax.axis_size("sp_1")
    at = jnp.stack([lax.axis_index("sp_0"), lax.axis_index("sp_1"), lax.axis_index("sp_2")])
    tok = query.shape[0]
    rows = tok * (query.shape[1] // HD)
    other_query = shifted(query, "sp_2", 1)
    pair = jnp.concatenate([keys, values], axis=1)
    ring = [pair] + [None] * (y_size - 1)
    down = up = pair
    for k in range(1, y_size // 2 + 1):
        down = ring[k] = shifted(down, "sp_1", 1)
        if k < y_size - k:
            up = ring[y_size - k] = shifted(up, "sp_1", -1)
    own_rows = jnp.stack(ring)
    (plane,) = call(
        functools.partial(assemble_kernel, y_size),
        [((2 * y_size, tok, 2 * HD), jnp.bfloat16)],
        (at, own_rows, shifted(own_rows, "sp_2", 1)),
        name="assemble",
    )
    scratch = [
        pltpu.VMEM((BK, BK), jnp.bfloat16),
        pltpu.VMEM((2, rows, BK), jnp.float32),
        pltpu.VMEM((2, rows, BK), jnp.bfloat16),
    ]
    state = ((rows, HD), jnp.float32)
    both_state = ((2 * rows, HD), jnp.float32)
    work = 2 * y_size * rows * BK * HD * 16
    doubled, own, own_total = call(
        own_plane_kernel,
        [((2 * rows, 2 * HD), jnp.bfloat16), state, state],
        (at, query, other_query, plane),
        scratch,
        work // 2,
        name="own",
    )
    acc = total = jnp.zeros(*both_state)
    done = own
    for k in range(1, z_size // 2 + 1):
        last = k == z_size // 2
        if k > 1:
            plane, done = lax.optimization_barrier((plane, done))
            if k == 2:
                own = done
            done = acc
        if last:
            upward = lax.axis_index("sp_2") == 0
            plane = jnp.where(upward, plane[y_size:], plane[:y_size])
        plane = counter_shifted(plane)
        acc, total = call(
            functools.partial(plane_kernel, k, z_size, tok, last),
            [((2, rows, HD), jnp.float32)] * 2 if last else [both_state] * 2,
            (at, doubled, plane, acc, total),
            [pltpu.VMEM((rows, HD), jnp.float32)] * 2 + scratch,
            work * 2,
            name="plane%d" % k,
        )
    theirs = shifted(jnp.stack([acc[1], total[1]]), "sp_2", 1)
    return call(
        merge_kernel,
        [((tok, query.shape[1]), jnp.bfloat16)],
        (at, own, own_total, acc, total, theirs[0], theirs[1]),
        name="merge",
    )[0]


def per_device(
    query,
    key_rows,
    value_rows,
    stream,
    out_weight,
    norm_gain,
    route_ids,
    route_weights,
    expert_gate,
    expert_up,
    expert_down,
    shared_gate,
    shared_up,
    shared_down,
):
    heads_out = attention(query, key_rows, value_rows)
    own_rows = stream.shape[0]
    token_heads = lax.all_to_all(heads_out, "tp", split_axis=0, concat_axis=1, tiled=True)
    attended = jnp.dot(
        token_heads,
        lax.all_gather(out_weight, "tp", axis=0, tiled=True),
        preferred_element_type=jnp.float32,
    )
    mid = (stream.astype(jnp.float32) + attended).astype(jnp.bfloat16)
    mid_wide = lax.optimization_barrier(mid).astype(jnp.float32)
    normed = (
        mid_wide
        * lax.rsqrt(jnp.mean(mid_wide * mid_wide, axis=1, keepdims=True) + 1e-06)
        * norm_gain
    ).astype(jnp.bfloat16)
    local_experts = expert_gate.shape[0]
    expert_count = lax.axis_size(SP) * local_experts
    capacity = 2 * own_rows * TOP_K // expert_count
    slot_count = expert_count * capacity
    flat_ids = route_ids.reshape(-1)
    membership = (flat_ids[:, None] == jnp.arange(expert_count, dtype=jnp.int32)[None, :]).astype(
        jnp.int32
    )
    before = jnp.cumsum(membership, axis=0) - membership
    slot_rank = jnp.sum(before * membership, axis=1)
    slot_ids = flat_ids * capacity + slot_rank
    placing = jnp.arange(slot_count, dtype=jnp.int32)[:, None] == slot_ids[None, :]
    dispatch = placing.reshape(slot_count, own_rows, TOP_K).any(axis=2).astype(jnp.bfloat16)
    outgoing = jnp.dot(dispatch, normed, preferred_element_type=jnp.float32).astype(jnp.bfloat16)
    outgoing = outgoing.reshape(lax.axis_size(SP), local_experts, capacity, D)
    arrived = lax.all_to_all(outgoing, SP, split_axis=0, concat_axis=0, tiled=True)
    gate_part = jnp.einsum(
        "sepd,edf->sepf", arrived, expert_gate, preferred_element_type=jnp.float32
    )
    up_part = jnp.einsum("sepd,edf->sepf", arrived, expert_up, preferred_element_type=jnp.float32)
    hidden = (jax.nn.silu(gate_part) * up_part).astype(jnp.bfloat16)
    produced = jnp.einsum(
        "sepf,efd->sepd", hidden, expert_down, preferred_element_type=jnp.float32
    ).astype(jnp.bfloat16)
    returned = lax.all_to_all(produced, SP, split_axis=0, concat_axis=0, tiled=True)
    returned = returned.reshape(slot_count, D)
    picking = (slot_ids[:, None] == jnp.arange(slot_count, dtype=jnp.int32)[None, :]).astype(
        jnp.bfloat16
    )
    selected_experts = jnp.dot(picking, returned, preferred_element_type=jnp.float32).reshape(
        own_rows, TOP_K, D
    )
    routed = jnp.sum(selected_experts * route_weights[:, :, None], axis=1)
    shared_hidden = (
        jax.nn.silu(jnp.dot(normed, shared_gate, preferred_element_type=jnp.float32))
        * jnp.dot(normed, shared_up, preferred_element_type=jnp.float32)
    ).astype(jnp.bfloat16)
    shared_out = jnp.dot(shared_hidden, shared_down, preferred_element_type=jnp.float32)
    return (mid_wide + routed + shared_out).astype(jnp.bfloat16)


def solution(mesh):
    split = Mesh(mesh.devices.reshape(8, 4, 2, mesh.shape["tp"]), ("sp_0", "sp_1", "sp_2", "tp"))
    in_specs = (
        P(SP, "tp"),
        P(SP, "tp"),
        P(SP, "tp"),
        P(SP_TP, None),
        P("tp", None),
        P(),
        P(SP_TP, None),
        P(SP_TP, None),
        P(SP, None, None),
        P(SP, None, None),
        P(SP, None, None),
        P(),
        P(),
        P(),
    )
    out_specs = P(SP_TP, None)
    return jax.shard_map(
        per_device, mesh=split, in_specs=in_specs, out_specs=out_specs, check_vma=False
    )
```

```python
import functools
import math

import jax
import jax.numpy as jnp
from jax import lax
from jax.experimental import pallas as pl
from jax.experimental.pallas import tpu as pltpu
from jax.sharding import Mesh
from jax.sharding import PartitionSpec as P


D = 2048
HD = 128
TOP_K = 4
SP = ("sp_0", "sp_1", "sp_2")
SP_TP = ("sp_0", "sp_1", "sp_2", "tp")


BK = 256
SCALE = math.log2(math.e) / math.sqrt(HD)


def shifted(value, axis, step):
    size = lax.axis_size(axis)
    return lax.ppermute(value, axis, [(i, (i + step) % size) for i in range(size)])


def counter_shifted(value):
    size = lax.axis_size("sp_0")
    pairs = [(2 * i, 2 * ((i + 1) % size)) for i in range(size)]
    pairs += [(2 * i + 1, 2 * ((i - 1) % size) + 1) for i in range(size)]
    return lax.ppermute(value, ("sp_0", "sp_2"), pairs)


def call(kernel, outs, args, scratch=(), flops=0):
    return pl.pallas_call(
        kernel,
        out_shape=[jax.ShapeDtypeStruct(*out) for out in outs],
        in_specs=[pl.BlockSpec(memory_space=pltpu.SMEM)]
        + [pl.BlockSpec(memory_space=pltpu.VMEM)] * (len(args) - 1),
        out_specs=[pl.BlockSpec(memory_space=pltpu.VMEM)] * len(outs),
        scratch_shapes=list(scratch),
        compiler_params=pltpu.CompilerParams(vmem_limit_bytes=24 * 2**20),
        cost_estimate=pl.CostEstimate(flops=flops, bytes_accessed=2**20, transcendentals=0),
    )(*args)


def assemble_kernel(y_size, at_ref, own_ref, other_ref, plane_ref):
    row, core = at_ref[1], at_ref[2]
    for k in range(y_size):
        place = (2 * ((row + y_size - k) % y_size) + y_size * core) % (2 * y_size)
        plane_ref[place + core] = own_ref[k]
        plane_ref[place + 1 - core] = other_ref[k]


def block_steps(
    q_ref, plane_ref, acc, carry, tri, level_buf, penalty_buf, first_row, tok, turn
):
    rows = acc.shape[0]
    shards = plane_ref.shape[0]

    def scores(j, slot, diagonal=False):
        keys = plane_ref[(j + turn) % shards, :, 0:HD]
        y = lax.dot_general(
            q_ref[pl.ds(first_row, rows), :],
            jnp.concatenate([keys, keys], axis=1),
            (((1,), (1,)), ((), ())),
            preferred_element_type=jnp.float32,
        )
        penalty = jnp.maximum(y, jnp.log2(1.0 + jnp.exp2(jnp.minimum(y, 126.0))))
        level = y - penalty
        if diagonal:
            query_at = lax.broadcasted_iota(jnp.int32, (rows, BK), 0) % tok
            visible = lax.broadcasted_iota(jnp.int32, (rows, BK), 1) < query_at
            penalty = jnp.where(visible, penalty, 0.0)
            level = jnp.where(visible, level, -1e30)
        level_buf[slot] = level
        penalty_buf[slot] = penalty.astype(jnp.bfloat16)

    def mix(j, slot):
        penalty = penalty_buf[slot]
        after = jnp.dot(penalty, tri[...], preferred_element_type=jnp.float32)
        so_far = carry[...]
        weights = jnp.exp2(level_buf[slot] - after - jnp.concatenate([so_far, so_far], axis=1))
        carry[...] = so_far + jnp.broadcast_to(
            after[:, 0:1] + penalty[:, 0:1].astype(jnp.float32), (rows, HD)
        )
        acc[...] += jnp.dot(
            weights.astype(jnp.bfloat16),
            plane_ref[(j + turn) % shards, :, HD : 2 * HD],
            preferred_element_type=jnp.float32,
        )

    def both(j, slot):
        mix(j, slot)
        scores(j - 1, 1 - slot)

    return scores, mix, both


def clear(acc, carry, tri):
    acc[...] = jnp.zeros_like(acc)
    carry[...] = jnp.zeros_like(carry)
    key_at = lax.broadcasted_iota(jnp.int32, (BK, BK), 0)
    later = key_at > lax.broadcasted_iota(jnp.int32, (BK, BK), 1)
    tri[...] = later.astype(jnp.float32).astype(jnp.bfloat16)


def own_plane_kernel(
    at_ref, own_ref, other_ref, plane_ref, q_ref, acc, carry, tri, level_buf, penalty_buf
):
    tok = own_ref.shape[0]
    heads = own_ref.shape[1] // HD
    rows = tok * heads
    core = at_ref[2]
    for place, ref in ((core, own_ref), (1 - core, other_ref)):
        for g in range(heads):
            scaled = ref[:, g * HD : (g + 1) * HD].astype(jnp.float32) * SCALE
            high = scaled.astype(jnp.bfloat16)
            target = pl.ds(pl.multiple_of(place * rows + g * tok, tok), tok)
            q_ref[target, 0:HD] = high
            q_ref[target, HD : 2 * HD] = (scaled - high.astype(jnp.float32)).astype(jnp.bfloat16)
    clear(acc, carry, tri)
    first_row = pl.multiple_of(core * rows, rows)
    scores, mix, both = block_steps(
        q_ref, plane_ref, acc, carry, tri, level_buf, penalty_buf, first_row, tok,
        plane_ref.shape[0] // 2 * core,
    )
    pos = 2 * at_ref[1] + core
    scores(pos, 0, diagonal=True)

    def step(i, _):
        both(pos - 2 * i, 0)
        both(pos - 2 * i - 1, 1)
        return 0

    lax.fori_loop(0, pos // 2, step, 0)

    @pl.when(pos % 2 == 1)
    def _():
        both(1, 0)
        mix(0, 1)

    @pl.when(pos % 2 == 0)
    def _():
        mix(0, 0)


def plane_kernel(
    distance, z_size, tok, last, at_ref, q_ref, plane_ref, acc_in, total_in, acc_out, total_out,
    acc, carry, tri, level_buf, penalty_buf
):
    rows = acc.shape[0]
    core = at_ref[2]
    below = jnp.where(core == 0, distance, z_size - distance)
    shards = plane_ref.shape[0]

    def part(h, _):
        first_row = pl.multiple_of(h * rows, rows)
        here = pl.ds(first_row, rows)
        clear(acc, carry, tri)

        @pl.when(below <= at_ref[0])
        def _():
            scores, mix, both = block_steps(
                q_ref, plane_ref, acc, carry, tri, level_buf, penalty_buf, first_row, tok,
                0 if last else shards // 2 * core,
            )
            scores(shards - 1, 0)

            def step(i, _):
                both(shards - 1 - 2 * i, 0)
                both(shards - 2 - 2 * i, 1)
                return 0

            lax.fori_loop(0, shards // 2 - 1, step, 0)
            both(1, 0)
            mix(0, 1)

        old, old_total = acc_in[here, :], total_in[here, :]
        new, new_total = acc[...], carry[...]
        upward = core == 0
        result = old * jnp.exp2(jnp.where(upward, 0.0, -new_total))
        result = result + new * jnp.exp2(jnp.where(upward, -old_total, 0.0))
        if last:
            place = jnp.where(h == core, 0, 1)
            acc_out[place] = result
            total_out[place] = old_total + new_total
        else:
            acc_out[here, :] = result
            total_out[here, :] = old_total + new_total
        return 0

    lax.fori_loop(0, 2, part, 0)


def merge_kernel(at_ref, own_ref, own_total, acc_ref, total_ref, theirs, their_total, out_ref):
    upward = at_ref[2] == 0
    tok = out_ref.shape[0]
    mine, other = acc_ref[0], theirs[...]
    newer_total = jnp.where(upward, total_ref[0], their_total[...])
    newer, older = jnp.where(upward, mine, other), jnp.where(upward, other, mine)
    mixed = own_ref[...] + jnp.exp2(-own_total[...]) * (newer + jnp.exp2(-newer_total) * older)
    for g in range(out_ref.shape[1] // HD):
        out_ref[:, g * HD : (g + 1) * HD] = mixed[g * tok : (g + 1) * tok].astype(out_ref.dtype)


def attention(at, query, keys, values):
    z_size, y_size = lax.axis_size("sp_0"), lax.axis_size("sp_1")
    tok = query.shape[0]
    rows = tok * (query.shape[1] // HD)
    other_query = shifted(query, "sp_2", 1)
    pair = jnp.concatenate([keys, values], axis=1)
    ring = [pair] + [None] * (y_size - 1)
    down = up = pair
    for k in range(1, y_size // 2 + 1):
        down = ring[k] = shifted(down, "sp_1", 1)
        if k < y_size - k:
            up = ring[y_size - k] = shifted(up, "sp_1", -1)
    own_rows = jnp.stack(ring)
    (plane,) = call(
        functools.partial(assemble_kernel, y_size),
        [((2 * y_size, tok, 2 * HD), jnp.bfloat16)],
        (at, own_rows, shifted(own_rows, "sp_2", 1)),
    )
    scratch = [
        pltpu.VMEM((BK, BK), jnp.bfloat16),
        pltpu.VMEM((2, rows, BK), jnp.float32),
        pltpu.VMEM((2, rows, BK), jnp.bfloat16),
    ]
    state = ((rows, HD), jnp.float32)
    both_state = ((2 * rows, HD), jnp.float32)
    work = 2 * y_size * rows * BK * HD * 16
    doubled, own, own_total = call(
        own_plane_kernel,
        [((2 * rows, 2 * HD), jnp.bfloat16), state, state],
        (at, query, other_query, plane),
        scratch,
        work // 2,
    )
    acc = total = jnp.zeros(*both_state)
    done = own
    for k in range(1, z_size // 2 + 1):
        last = k == z_size // 2
        if k > 1:
            plane, done = lax.optimization_barrier((plane, done))
            if k == 2:
                own = done
            done = acc
        if last:
            plane = plane[y_size:]
        plane = counter_shifted(plane)
        acc, total = call(
            functools.partial(plane_kernel, k, z_size, tok, last),
            [((2, rows, HD), jnp.float32)] * 2 if last else [both_state] * 2,
            (at, doubled, plane, acc, total),
            [pltpu.VMEM((rows, HD), jnp.float32)] * 2 + scratch,
            work * 2,
        )
    theirs = shifted(jnp.stack([acc[1], total[1]]), "sp_2", 1)
    return call(
        merge_kernel,
        [((tok, query.shape[1]), jnp.bfloat16)],
        (at, own, own_total, acc, total, theirs[0], theirs[1]),
    )[0]


def chosen_slots(slots, weights, count):
    slot = lax.broadcasted_iota(jnp.int32, (slots.shape[0], count), 1)
    picked = jnp.zeros(slot.shape, jnp.float32)
    for k in range(slots.shape[1]):
        picked += jnp.where(slot == slots[:, k : k + 1], weights[:, k : k + 1], 0.0)
    return picked


def project_kernel(
    at_ref, heads_ref, w0, w1, w2, w3, stream_ref, gain_ref, slots_ref, mid_ref, normed_ref, out_ref
):
    weights = (w0, w1, w2, w3)
    own = at_ref[3]
    attended = jnp.zeros(stream_ref.shape, jnp.float32)
    for k, weight in enumerate(weights):
        source = (own + len(weights) - k) % len(weights)
        attended += jnp.dot(heads_ref[source], weight[...], preferred_element_type=jnp.float32)
    mid = (stream_ref[...].astype(jnp.float32) + attended).astype(jnp.bfloat16)
    mid_ref[...] = mid
    wide = mid.astype(jnp.float32)
    scale = lax.rsqrt(jnp.mean(wide * wide, axis=1, keepdims=True) + 1e-06)
    normed = (wide * scale * gain_ref[...]).astype(jnp.bfloat16)
    normed_ref[...] = normed
    ones = jnp.ones(slots_ref.shape, jnp.float32)
    picked = chosen_slots(slots_ref[...], ones, out_ref.shape[0]).astype(jnp.bfloat16)
    out_ref[...] = lax.dot_general(
        picked, normed, (((0,), (0,)), ((), ())), preferred_element_type=jnp.float32
    ).astype(jnp.bfloat16)


def gated(rows, gate, up):
    gate_part = jnp.dot(rows, gate, preferred_element_type=jnp.float32)
    up_part = jnp.dot(rows, up, preferred_element_type=jnp.float32)
    return (gate_part / (1.0 + jnp.exp(-gate_part)) * up_part).astype(jnp.bfloat16)


def expert_kernel(at_ref, rows_ref, gate_ref, up_ref, down_ref, out_ref):
    chunk = 256

    def part(k, _):
        here = pl.ds(pl.multiple_of(k * chunk, chunk), chunk)
        hidden = gated(rows_ref[here, :], gate_ref[...], up_ref[...])
        out_ref[here, :] = jnp.dot(
            hidden, down_ref[...], preferred_element_type=jnp.float32
        ).astype(jnp.bfloat16)
        return 0

    lax.fori_loop(0, rows_ref.shape[0] // chunk, part, 0)


def shared_kernel(at_ref, normed_ref, mid_ref, gate_ref, up_ref, down_ref, base_ref):
    hidden = gated(normed_ref[...], gate_ref[...], up_ref[...])
    base_ref[...] = mid_ref[...].astype(jnp.float32) + jnp.dot(
        hidden, down_ref[...], preferred_element_type=jnp.float32
    )


def combine_kernel(at_ref, base_ref, rows_ref, slots_ref, weights_ref, out_ref):
    picked = chosen_slots(slots_ref[...], weights_ref[...], rows_ref.shape[0])
    high = picked.astype(jnp.bfloat16)
    low = (picked - high.astype(jnp.float32)).astype(jnp.bfloat16)
    routed = jnp.dot(high, rows_ref[...], preferred_element_type=jnp.float32)
    routed += jnp.dot(low, rows_ref[...], preferred_element_type=jnp.float32)
    out_ref[...] = (base_ref[...] + routed).astype(jnp.bfloat16)


def per_device(
    query,
    key_rows,
    value_rows,
    stream,
    out_weight,
    norm_gain,
    route_ids,
    route_weights,
    expert_gate,
    expert_up,
    expert_down,
    shared_gate,
    shared_up,
    shared_down,
):
    at = jnp.stack([lax.axis_index(axis) for axis in SP_TP])
    weight_below = shifted(out_weight, "tp", 1)
    weight_above = shifted(out_weight, "tp", -1)
    weight_far = shifted(weight_below, "tp", 1)
    out_weights = (out_weight, weight_below, weight_far, weight_above)
    own_rows = stream.shape[0]
    expert_count = lax.axis_size(SP) * expert_gate.shape[0]
    capacity = 2 * own_rows * TOP_K // expert_count
    slot_count = expert_count * capacity
    flat_ids = route_ids.reshape(-1)
    membership = (flat_ids[:, None] == jnp.arange(expert_count, dtype=jnp.int32)[None, :]).astype(
        jnp.int32
    )
    before = jnp.cumsum(membership, axis=0) - membership
    slot_rank = jnp.sum(before * membership, axis=1)
    slots = (flat_ids * capacity + slot_rank).reshape(route_ids.shape)
    heads_out = attention(at, query, key_rows, value_rows)
    token_heads = lax.all_to_all(
        heads_out.reshape(-1, own_rows, heads_out.shape[1]), "tp", 0, 0, tiled=True
    )
    wide = (own_rows, D)
    mid, normed, outgoing = call(
        project_kernel,
        [(wide, jnp.bfloat16), (wide, jnp.bfloat16), ((slot_count, D), jnp.bfloat16)],
        (at, token_heads, *out_weights, stream, norm_gain.reshape(1, D), slots),
        flops=2**29,
    )
    exchange = (lax.axis_size(SP), slot_count // lax.axis_size(SP), D)
    arrived = lax.all_to_all(outgoing.reshape(exchange), SP, 0, 0, tiled=True)
    (produced,) = call(
        expert_kernel,
        [((slot_count, D), jnp.bfloat16)],
        (at, arrived.reshape(slot_count, D), expert_gate[0], expert_up[0], expert_down[0]),
        flops=2**32,
    )
    returned = lax.all_to_all(produced.reshape(exchange), SP, 0, 0, tiled=True)
    (base,) = call(
        shared_kernel,
        [(wide, jnp.float32)],
        (at, normed, mid, shared_gate, shared_up, shared_down),
        flops=2**30,
    )
    return call(
        combine_kernel,
        [(wide, jnp.bfloat16)],
        (at, base, returned.reshape(slot_count, D), slots, route_weights),
        flops=2**28,
    )[0]


def solution(mesh):
    split = Mesh(mesh.devices.reshape(8, 4, 2, mesh.shape["tp"]), ("sp_0", "sp_1", "sp_2", "tp"))
    in_specs = (
        P(SP, "tp"),
        P(SP, "tp"),
        P(SP, "tp"),
        P(SP_TP, None),
        P("tp", None),
        P(),
        P(SP_TP, None),
        P(SP_TP, None),
        P(SP, None, None),
        P(SP, None, None),
        P(SP, None, None),
        P(),
        P(),
        P(),
    )
    out_specs = P(SP_TP, None)

    return jax.shard_map(
        per_device, mesh=split, in_specs=in_specs, out_specs=out_specs, check_vma=False
    )
```

```python
import functools
import math

import jax
import jax.numpy as jnp
from jax import lax
from jax.experimental import pallas as pl
from jax.experimental.pallas import tpu as pltpu
from jax.sharding import Mesh
from jax.sharding import PartitionSpec as P


D = 2048
HD = 128
TOP_K = 4
SP = ("sp_0", "sp_1", "sp_2")
SP_TP = ("sp_0", "sp_1", "sp_2", "tp")


BK = 256
SCALE = math.log2(math.e) / math.sqrt(HD)


def shifted(value, axis, step):
    size = lax.axis_size(axis)
    return lax.ppermute(value, axis, [(i, (i + step) % size) for i in range(size)])


def counter_shifted(value):
    size = lax.axis_size("sp_0")
    pairs = [(2 * i, 2 * ((i + 1) % size)) for i in range(size)]
    pairs += [(2 * i + 1, 2 * ((i - 1) % size) + 1) for i in range(size)]
    return lax.ppermute(value, ("sp_0", "sp_2"), pairs)


def call(kernel, outs, args, scratch=(), flops=0):
    return pl.pallas_call(
        kernel,
        out_shape=[jax.ShapeDtypeStruct(*out) for out in outs],
        in_specs=[pl.BlockSpec(memory_space=pltpu.SMEM)]
        + [pl.BlockSpec(memory_space=pltpu.VMEM)] * (len(args) - 1),
        out_specs=[pl.BlockSpec(memory_space=pltpu.VMEM)] * len(outs),
        scratch_shapes=list(scratch),
        compiler_params=pltpu.CompilerParams(vmem_limit_bytes=24 * 2**20),
        cost_estimate=pl.CostEstimate(flops=flops, bytes_accessed=2**20, transcendentals=0),
    )(*args)


def assemble_kernel(at_ref, own_ref, other_ref, half_ref):
    row, core = at_ref[1] % 2, at_ref[2]
    for k in range(2):
        place = 2 * jnp.where(row == k, 0, 1)
        half_ref[place + core] = own_ref[k]
        half_ref[place + 1 - core] = other_ref[k]


def join_halves(at_ref, half_ref, across_ref, plane):
    shards = half_ref.shape[0]
    upper = at_ref[1] // 2
    for k in range(shards):
        plane[upper * shards + k] = half_ref[k]
        plane[(1 - upper) * shards + k] = across_ref[k]


def block_steps(q_ref, plane_ref, acc, carry, tri, level_buf, penalty_buf, first_row, tok):
    rows = acc.shape[0]

    def scores(j, slot, diagonal=False):
        keys = plane_ref[j, :, 0:HD]
        y = lax.dot_general(
            q_ref[pl.ds(first_row, rows), :],
            jnp.concatenate([keys, keys], axis=1),
            (((1,), (1,)), ((), ())),
            preferred_element_type=jnp.float32,
        )
        penalty = jnp.maximum(y, jnp.log2(1.0 + jnp.exp2(jnp.minimum(y, 126.0))))
        level = y - penalty
        if diagonal:
            query_at = lax.broadcasted_iota(jnp.int32, (rows, BK), 0) % tok
            visible = lax.broadcasted_iota(jnp.int32, (rows, BK), 1) < query_at
            penalty = jnp.where(visible, penalty, 0.0)
            level = jnp.where(visible, level, -1e30)
        level_buf[slot] = level
        penalty_buf[slot] = penalty.astype(jnp.bfloat16)

    def mix(j, slot):
        penalty = penalty_buf[slot]
        after = jnp.dot(penalty, tri[...], preferred_element_type=jnp.float32)
        so_far = carry[...]
        weights = jnp.exp2(level_buf[slot] - after - jnp.concatenate([so_far, so_far], axis=1))
        carry[...] = so_far + jnp.broadcast_to(
            after[:, 0:1] + penalty[:, 0:1].astype(jnp.float32), (rows, HD)
        )
        acc[...] += jnp.dot(
            weights.astype(jnp.bfloat16),
            plane_ref[j, :, HD : 2 * HD],
            preferred_element_type=jnp.float32,
        )

    def both(j, slot):
        mix(j, slot)
        scores(j - 1, 1 - slot)

    return scores, mix, both


def clear(acc, carry, tri):
    acc[...] = jnp.zeros_like(acc)
    carry[...] = jnp.zeros_like(carry)
    key_at = lax.broadcasted_iota(jnp.int32, (BK, BK), 0)
    later = key_at > lax.broadcasted_iota(jnp.int32, (BK, BK), 1)
    tri[...] = later.astype(jnp.float32).astype(jnp.bfloat16)


def own_plane_kernel(
    at_ref, own_ref, other_ref, half_ref, across_ref, q_ref, acc, carry,
    tri, level_buf, penalty_buf, plane,
):
    tok = own_ref.shape[0]
    heads = own_ref.shape[1] // HD
    rows = tok * heads
    core = at_ref[2]
    for place, ref in ((core, own_ref), (1 - core, other_ref)):
        for g in range(heads):
            scaled = ref[:, g * HD : (g + 1) * HD].astype(jnp.float32) * SCALE
            high = scaled.astype(jnp.bfloat16)
            target = pl.ds(pl.multiple_of(place * rows + g * tok, tok), tok)
            q_ref[target, 0:HD] = high
            q_ref[target, HD : 2 * HD] = (scaled - high.astype(jnp.float32)).astype(jnp.bfloat16)
    clear(acc, carry, tri)
    join_halves(at_ref, half_ref, across_ref, plane)
    first_row = pl.multiple_of(core * rows, rows)
    scores, mix, both = block_steps(
        q_ref, plane, acc, carry, tri, level_buf, penalty_buf, first_row, tok
    )
    pos = 2 * at_ref[1] + core
    scores(pos, 0, diagonal=True)

    def step(i, _):
        both(pos - 2 * i, 0)
        both(pos - 2 * i - 1, 1)
        return 0

    lax.fori_loop(0, pos // 2, step, 0)

    @pl.when(pos % 2 == 1)
    def _():
        both(1, 0)
        mix(0, 1)

    @pl.when(pos % 2 == 0)
    def _():
        mix(0, 0)


def plane_kernel(
    distance, z_size, tok, last, at_ref, q_ref, half_ref, across_ref, acc_in, total_in, *refs
):
    outs, (acc, carry, tri, level_buf, penalty_buf, plane) = refs[:2], refs[2:]
    rows = acc.shape[0]
    core = at_ref[2]
    below = jnp.where(core == 0, distance, z_size - distance)
    visible = below <= at_ref[0]
    shards = half_ref.shape[0] if last else 2 * half_ref.shape[0]
    upward = core == 0

    @pl.when(visible)
    def _():
        if last:
            direct = (at_ref[1] // 2) == 1 - core
            for k in range(shards):
                plane[k] = jnp.where(direct, half_ref[k], across_ref[k])
        else:
            join_halves(at_ref, half_ref, across_ref, plane)

    def part(h, _):
        first_row = pl.multiple_of(h * rows, rows)
        here = pl.ds(first_row, rows)
        clear(acc, carry, tri)

        @pl.when(visible)
        def _():
            scores, mix, both = block_steps(
                q_ref, plane, acc, carry, tri, level_buf, penalty_buf, first_row, tok
            )
            scores(shards - 1, 0)

            def step(i, _):
                both(shards - 1 - 2 * i, 0)
                both(shards - 2 - 2 * i, 1)
                return 0

            lax.fori_loop(0, shards // 2 - 1, step, 0)
            both(1, 0)
            mix(0, 1)

        old, old_total = acc_in[here, :], total_in[here, :]
        new, new_total = acc[...], carry[...]
        result = old * jnp.exp2(jnp.where(upward, 0.0, -new_total))
        result = result + new * jnp.exp2(jnp.where(upward, -old_total, 0.0))
        total = old_total + new_total
        if last:
            for owned, out in ((True, outs[0]), (False, outs[1])):

                @pl.when((h == core) == owned)
                def _(out=out):
                    out[0] = result
                    out[1] = total
        else:
            outs[0][here, :] = result
            outs[1][here, :] = total
        return 0

    lax.fori_loop(0, 2, part, 0)


def merge_kernel(at_ref, own_ref, own_total, mine, theirs, out_ref):
    upward = at_ref[2] == 0
    tok = out_ref.shape[0]
    newer_total = jnp.where(upward, mine[1], theirs[1])
    newer, older = jnp.where(upward, mine[0], theirs[0]), jnp.where(upward, theirs[0], mine[0])
    mixed = own_ref[...] + jnp.exp2(-own_total[...]) * (newer + jnp.exp2(-newer_total) * older)
    for g in range(out_ref.shape[1] // HD):
        out_ref[:, g * HD : (g + 1) * HD] = mixed[g * tok : (g + 1) * tok].astype(out_ref.dtype)


def attention(at, query, keys, values):
    z_size, y_size = lax.axis_size("sp_0"), lax.axis_size("sp_1")
    tok = query.shape[0]
    rows = tok * (query.shape[1] // HD)
    pair = jnp.concatenate([keys, values], axis=1)
    near = lax.ppermute(pair, "sp_1", [(i, i ^ 1) for i in range(y_size)])
    own_rows = jnp.stack([pair, near])
    (half,) = call(
        assemble_kernel,
        [((y_size, tok, 2 * HD), jnp.bfloat16)],
        (at, own_rows, shifted(own_rows, "sp_2", 1)),
    )

    def from_across(value):
        return lax.ppermute(value, "sp_1", [(i, y_size - 1 - i) for i in range(y_size)])

    scratch = [
        pltpu.VMEM((BK, BK), jnp.bfloat16),
        pltpu.VMEM((2, rows, BK), jnp.float32),
        pltpu.VMEM((2, rows, BK), jnp.bfloat16),
        pltpu.VMEM((2 * y_size, tok, 2 * HD), jnp.bfloat16),
    ]
    state = ((rows, HD), jnp.float32)
    both_state = ((2 * rows, HD), jnp.float32)
    work = 2 * y_size * rows * BK * HD * 16
    across = from_across(half)
    other_query = shifted(query, "sp_2", 1)
    doubled, own, own_total = call(
        own_plane_kernel,
        [((2 * rows, 2 * HD), jnp.bfloat16), state, state],
        (at, query, other_query, half, across),
        scratch,
        work // 2,
    )
    acc = total = jnp.zeros(*both_state)
    for k in range(1, z_size // 2 + 1):
        last = k == z_size // 2
        if k == 3:
            half, own = lax.optimization_barrier((half, own))
        if k == 4:
            half, before = lax.optimization_barrier((half, before))
        half = counter_shifted(half)
        across = from_across(half)
        acc, total = call(
            functools.partial(plane_kernel, k, z_size, tok, last),
            [((2, rows, HD), jnp.float32)] * 2 if last else [both_state] * 2,
            (at, doubled, half, across, acc, total),
            [pltpu.VMEM((rows, HD), jnp.float32)] * 2 + scratch,
            work * 2,
        )
        if k == 1:
            before = acc
    return call(
        merge_kernel,
        [((tok, query.shape[1]), jnp.bfloat16)],
        (at, own, own_total, acc, shifted(total, "sp_2", 1)),
    )[0]


def chosen_slots(slots, weights, count):
    slot = lax.broadcasted_iota(jnp.int32, (slots.shape[0], count), 1)
    picked = jnp.zeros(slot.shape, jnp.float32)
    for k in range(slots.shape[1]):
        picked += jnp.where(slot == slots[:, k : k + 1], weights[:, k : k + 1], 0.0)
    return picked


def project_kernel(
    at_ref, heads_ref, w0, w1, w2, w3, stream_ref, gain_ref, slots_ref, mid_ref, normed_ref, out_ref
):
    weights = (w0, w1, w2, w3)
    own = at_ref[3]
    attended = jnp.zeros(stream_ref.shape, jnp.float32)
    for k, weight in enumerate(weights):
        source = (own + len(weights) - k) % len(weights)
        attended += jnp.dot(heads_ref[source], weight[...], preferred_element_type=jnp.float32)
    mid = (stream_ref[...].astype(jnp.float32) + attended).astype(jnp.bfloat16)
    mid_ref[...] = mid
    wide = mid.astype(jnp.float32)
    scale = lax.rsqrt(jnp.mean(wide * wide, axis=1, keepdims=True) + 1e-06)
    normed = (wide * scale * gain_ref[...]).astype(jnp.bfloat16)
    normed_ref[...] = normed
    ones = jnp.ones(slots_ref.shape, jnp.float32)
    picked = chosen_slots(slots_ref[...], ones, out_ref.shape[0]).astype(jnp.bfloat16)
    out_ref[...] = lax.dot_general(
        picked, normed, (((0,), (0,)), ((), ())), preferred_element_type=jnp.float32
    ).astype(jnp.bfloat16)


def gated(rows, gate, up):
    gate_part = jnp.dot(rows, gate, preferred_element_type=jnp.float32)
    up_part = jnp.dot(rows, up, preferred_element_type=jnp.float32)
    return (gate_part / (1.0 + jnp.exp(-gate_part)) * up_part).astype(jnp.bfloat16)


def expert_kernel(at_ref, rows_ref, gate_ref, up_ref, down_ref, out_ref):
    chunk = 256

    def part(k, _):
        here = pl.ds(pl.multiple_of(k * chunk, chunk), chunk)
        hidden = gated(rows_ref[here, :], gate_ref[...], up_ref[...])
        out_ref[here, :] = jnp.dot(
            hidden, down_ref[...], preferred_element_type=jnp.float32
        ).astype(jnp.bfloat16)
        return 0

    lax.fori_loop(0, rows_ref.shape[0] // chunk, part, 0)


def shared_kernel(at_ref, normed_ref, mid_ref, gate_ref, up_ref, down_ref, base_ref):
    hidden = gated(normed_ref[...], gate_ref[...], up_ref[...])
    base_ref[...] = mid_ref[...].astype(jnp.float32) + jnp.dot(
        hidden, down_ref[...], preferred_element_type=jnp.float32
    )


def combine_kernel(at_ref, base_ref, rows_ref, slots_ref, weights_ref, out_ref):
    picked = chosen_slots(slots_ref[...], weights_ref[...], rows_ref.shape[0])
    high = picked.astype(jnp.bfloat16)
    low = (picked - high.astype(jnp.float32)).astype(jnp.bfloat16)
    routed = jnp.dot(high, rows_ref[...], preferred_element_type=jnp.float32)
    routed += jnp.dot(low, rows_ref[...], preferred_element_type=jnp.float32)
    out_ref[...] = (base_ref[...] + routed).astype(jnp.bfloat16)


def per_device(
    query,
    key_rows,
    value_rows,
    stream,
    out_weight,
    norm_gain,
    route_ids,
    route_weights,
    expert_gate,
    expert_up,
    expert_down,
    shared_gate,
    shared_up,
    shared_down,
):
    at = jnp.stack([lax.axis_index(axis) for axis in SP_TP])
    weight_below = shifted(out_weight, "tp", 1)
    weight_above = shifted(out_weight, "tp", -1)
    weight_far = shifted(weight_below, "tp", 1)
    out_weights = (out_weight, weight_below, weight_far, weight_above)
    own_rows = stream.shape[0]
    expert_count = lax.axis_size(SP) * expert_gate.shape[0]
    capacity = 2 * own_rows * TOP_K // expert_count
    slot_count = expert_count * capacity
    flat_ids = route_ids.reshape(-1)
    membership = (flat_ids[:, None] == jnp.arange(expert_count, dtype=jnp.int32)[None, :]).astype(
        jnp.int32
    )
    before = jnp.cumsum(membership, axis=0) - membership
    slot_rank = jnp.sum(before * membership, axis=1)
    slots = (flat_ids * capacity + slot_rank).reshape(route_ids.shape)
    heads_out = attention(at, query, key_rows, value_rows)
    token_heads = lax.all_to_all(
        heads_out.reshape(-1, own_rows, heads_out.shape[1]), "tp", 0, 0, tiled=True
    )
    wide = (own_rows, D)
    mid, normed, outgoing = call(
        project_kernel,
        [(wide, jnp.bfloat16), (wide, jnp.bfloat16), ((slot_count, D), jnp.bfloat16)],
        (at, token_heads, *out_weights, stream, norm_gain.reshape(1, D), slots),
        flops=2**29,
    )
    exchange = (lax.axis_size(SP), slot_count // lax.axis_size(SP), D)
    arrived = lax.all_to_all(outgoing.reshape(exchange), SP, 0, 0, tiled=True)
    (produced,) = call(
        expert_kernel,
        [((slot_count, D), jnp.bfloat16)],
        (at, arrived.reshape(slot_count, D), expert_gate[0], expert_up[0], expert_down[0]),
        flops=2**32,
    )
    returned = lax.all_to_all(produced.reshape(exchange), SP, 0, 0, tiled=True)
    (base,) = call(
        shared_kernel,
        [(wide, jnp.float32)],
        (at, normed, mid, shared_gate, shared_up, shared_down),
        flops=2**30,
    )
    return call(
        combine_kernel,
        [(wide, jnp.bfloat16)],
        (at, base, returned.reshape(slot_count, D), slots, route_weights),
        flops=2**28,
    )[0]


def solution(mesh):
    split = Mesh(mesh.devices.reshape(8, 4, 2, mesh.shape["tp"]), ("sp_0", "sp_1", "sp_2", "tp"))
    in_specs = (
        P(SP, "tp"),
        P(SP, "tp"),
        P(SP, "tp"),
        P(SP_TP, None),
        P("tp", None),
        P(),
        P(SP_TP, None),
        P(SP_TP, None),
        P(SP, None, None),
        P(SP, None, None),
        P(SP, None, None),
        P(),
        P(),
        P(),
    )
    out_specs = P(SP_TP, None)

    return jax.shard_map(
        per_device, mesh=split, in_specs=in_specs, out_specs=out_specs, check_vma=False
    )
```

```python
import functools
import math

import jax
import jax.numpy as jnp
from jax import lax
from jax.experimental import pallas as pl
from jax.experimental.pallas import tpu as pltpu
from jax.sharding import Mesh
from jax.sharding import PartitionSpec as P


D = 2048
HD = 128
TOP_K = 4
SP = ("sp_0", "sp_1", "sp_2")
SP_TP = ("sp_0", "sp_1", "sp_2", "tp")


BK = 256
SCALE = math.log2(math.e) / math.sqrt(HD)


def shifted(value, axis, step):
    size = lax.axis_size(axis)
    return lax.ppermute(value, axis, [(i, (i + step) % size) for i in range(size)])


def counter_shifted(value):
    size = lax.axis_size("sp_0")
    pairs = [(2 * i, 2 * ((i + 1) % size)) for i in range(size)]
    pairs += [(2 * i + 1, 2 * ((i - 1) % size) + 1) for i in range(size)]
    return lax.ppermute(value, ("sp_0", "sp_2"), pairs)


def call(kernel, outs, args, scratch=(), flops=0):
    near = pl.BlockSpec(memory_space=pltpu.VMEM)
    return pl.pallas_call(
        kernel,
        out_shape=[jax.ShapeDtypeStruct(*out) for out in outs],
        in_specs=[pl.BlockSpec(memory_space=pltpu.SMEM)]
        + [near] * (len(args) - 1),
        out_specs=[near] * len(outs),
        scratch_shapes=list(scratch),
        compiler_params=pltpu.CompilerParams(vmem_limit_bytes=24 * 2**20),
        cost_estimate=pl.CostEstimate(flops=flops, bytes_accessed=2**20, transcendentals=0),
    )(*args)


def assemble_kernel(at_ref, own_ref, other_ref, half_ref):
    row, core = at_ref[1] % 2, at_ref[2]
    for k in range(2):
        place = 2 * jnp.where(row == k, 0, 1)
        half_ref[place + core] = own_ref[k]
        half_ref[place + 1 - core] = other_ref[k]


def join_halves(at_ref, half_ref, across_ref, plane):
    shards = half_ref.shape[0]
    upper = at_ref[1] // 2
    for k in range(shards):
        plane[upper * shards + k] = half_ref[k]
        plane[(1 - upper) * shards + k] = across_ref[k]


def block_steps(q_ref, plane_ref, acc, carry, tri, level_buf, penalty_buf, first_row, tok):
    rows = acc.shape[0]

    def scores(j, slot, diagonal=False):
        keys = plane_ref[j, :, 0:HD]
        y = lax.dot_general(
            q_ref[pl.ds(first_row, rows), :],
            jnp.concatenate([keys, keys], axis=1),
            (((1,), (1,)), ((), ())),
            preferred_element_type=jnp.float32,
        )
        penalty = jnp.maximum(y, jnp.log2(1.0 + jnp.exp2(jnp.minimum(y, 126.0))))
        level = y - penalty
        if diagonal:
            query_at = lax.broadcasted_iota(jnp.int32, (rows, BK), 0) % tok
            visible = lax.broadcasted_iota(jnp.int32, (rows, BK), 1) < query_at
            penalty = jnp.where(visible, penalty, 0.0)
            level = jnp.where(visible, level, -1e30)
        level_buf[slot] = level
        penalty_buf[slot] = penalty.astype(jnp.bfloat16)

    def mix(j, slot):
        penalty = penalty_buf[slot]
        after = jnp.dot(penalty, tri[...], preferred_element_type=jnp.float32)
        so_far = carry[...]
        weights = jnp.exp2(level_buf[slot] - after - jnp.concatenate([so_far, so_far], axis=1))
        carry[...] = so_far + jnp.broadcast_to(
            after[:, 0:1] + penalty[:, 0:1].astype(jnp.float32), (rows, HD)
        )
        acc[...] += jnp.dot(
            weights.astype(jnp.bfloat16),
            plane_ref[j, :, HD : 2 * HD],
            preferred_element_type=jnp.float32,
        )

    def both(j, slot):
        mix(j, slot)
        scores(j - 1, 1 - slot)

    return scores, mix, both


def clear(acc, carry, tri):
    acc[...] = jnp.zeros_like(acc)
    carry[...] = jnp.zeros_like(carry)
    key_at = lax.broadcasted_iota(jnp.int32, (BK, BK), 0)
    later = key_at > lax.broadcasted_iota(jnp.int32, (BK, BK), 1)
    tri[...] = later.astype(jnp.float32).astype(jnp.bfloat16)


def scale_queries(at_ref, own_ref, other_ref, q_ref):
    tok = own_ref.shape[0]
    heads = own_ref.shape[1] // HD
    core = at_ref[2]
    for place, ref in ((core, own_ref), (1 - core, other_ref)):
        for g in range(heads):
            scaled = ref[:, g * HD : (g + 1) * HD].astype(jnp.float32) * SCALE
            high = scaled.astype(jnp.bfloat16)
            target = pl.ds(pl.multiple_of(place * tok * heads + g * tok, tok), tok)
            q_ref[target, 0:HD] = high
            q_ref[target, HD : 2 * HD] = (scaled - high.astype(jnp.float32)).astype(jnp.bfloat16)


def own_plane_kernel(
    at_ref, own_ref, other_ref, half_ref, across_ref, out_ref,
    q_buf, acc, carry, tri, level_buf, penalty_buf, plane,
):
    rows = acc.shape[0]
    core = at_ref[2]
    scale_queries(at_ref, own_ref, other_ref, q_buf)
    clear(acc, carry, tri)
    join_halves(at_ref, half_ref, across_ref, plane)
    first_row = pl.multiple_of(core * rows, rows)
    scores, mix, both = block_steps(
        q_buf, plane, acc, carry, tri, level_buf, penalty_buf, first_row, own_ref.shape[0]
    )
    pos = 2 * at_ref[1] + core
    scores(pos, 0, diagonal=True)

    def step(i, _):
        both(pos - 2 * i, 0)
        both(pos - 2 * i - 1, 1)
        return 0

    lax.fori_loop(0, pos // 2, step, 0)

    @pl.when(pos % 2 == 1)
    def _():
        both(1, 0)
        mix(0, 1)

    @pl.when(pos % 2 == 0)
    def _():
        mix(0, 0)

    out_ref[0] = acc[...]
    out_ref[1] = carry[...]


def plane_kernel(distance, z_size, first, last, at_ref, own_ref, other_ref, *refs):
    half_ref, across_ref, *refs = refs
    if not first:
        state, *refs = refs
    if last:
        closest, mine_ref, theirs_ref, *refs = refs
    else:
        out_ref, *refs = refs
    q_buf, acc, carry, tri, level_buf, penalty_buf, plane = refs
    rows = acc.shape[0]
    core = at_ref[2]
    below = jnp.where(core == 0, distance, z_size - distance)
    visible = below <= at_ref[0]
    shards = half_ref.shape[0] if last else 2 * half_ref.shape[0]
    upward = core == 0

    @pl.when(visible)
    def _():
        scale_queries(at_ref, own_ref, other_ref, q_buf)
        if last:
            direct = (at_ref[1] // 2) == 1 - core
            for k in range(shards):
                plane[k] = jnp.where(direct, half_ref[k], across_ref[k])
        else:
            join_halves(at_ref, half_ref, across_ref, plane)

    def part(turn, _):
        first_row = pl.multiple_of(jnp.where(turn == 0, 1 - core, core) * rows, rows)
        here = pl.ds(first_row, rows)
        clear(acc, carry, tri)

        @pl.when(visible)
        def _():
            scores, mix, both = block_steps(
                q_buf, plane, acc, carry, tri, level_buf, penalty_buf, first_row,
                own_ref.shape[0],
            )
            scores(shards - 1, 0)

            def step(i, _):
                both(shards - 1 - 2 * i, 0)
                both(shards - 2 - 2 * i, 1)
                return 0

            lax.fori_loop(0, shards // 2 - 1, step, 0)
            both(1, 0)
            mix(0, 1)

        result, total = acc[...], carry[...]
        if not first:
            old, old_total = state[0, here, :], state[1, here, :]
            result = result * jnp.exp2(jnp.where(upward, -old_total, 0.0))
            result = result + old * jnp.exp2(jnp.where(upward, 0.0, -total))
            total = total + old_total
        if not last:
            out_ref[0, here, :] = result
            out_ref[1, here, :] = total
            return 0

        @pl.when(turn == 0)
        def _():
            theirs_ref[0] = result
            theirs_ref[1] = total

        @pl.when(turn == 1)
        def _():
            left = jnp.exp2(-closest[1])
            mine_ref[0] = closest[0] + jnp.where(upward, left * result, 0.0)
            mine_ref[1] = jnp.where(upward, left * jnp.exp2(-total), left)
            mine_ref[2] = jnp.where(upward, 0.0, left * result)

        return 0

    lax.fori_loop(0, 2, part, 0)


def merge_kernel(at_ref, mine, theirs, out_ref):
    upward = at_ref[2] == 0
    tok = out_ref.shape[0]
    older = jnp.where(upward, 0.0, jnp.exp2(-theirs[1])) * mine[2]
    mixed = mine[0] + mine[1] * theirs[0] + older
    for g in range(out_ref.shape[1] // HD):
        out_ref[:, g * HD : (g + 1) * HD] = mixed[g * tok : (g + 1) * tok].astype(out_ref.dtype)


def attention(at, query, keys, values):
    z_size, y_size = lax.axis_size("sp_0"), lax.axis_size("sp_1")
    tok = query.shape[0]
    rows = tok * (query.shape[1] // HD)
    pair = jnp.concatenate([keys, values], axis=1)
    near = lax.ppermute(pair, "sp_1", [(i, i ^ 1) for i in range(y_size)])
    own_rows = jnp.stack([pair, near])
    (half,) = call(
        assemble_kernel,
        [((y_size, tok, 2 * HD), jnp.bfloat16)],
        (at, own_rows, shifted(own_rows, "sp_2", 1)),
    )

    def from_across(value):
        return lax.ppermute(value, "sp_1", [(i, y_size - 1 - i) for i in range(y_size)])

    scratch = [
        pltpu.VMEM((2 * rows, 2 * HD), jnp.bfloat16),
        pltpu.VMEM((rows, HD), jnp.float32),
        pltpu.VMEM((rows, HD), jnp.float32),
        pltpu.VMEM((BK, BK), jnp.bfloat16),
        pltpu.VMEM((2, rows, BK), jnp.float32),
        pltpu.VMEM((2, rows, BK), jnp.bfloat16),
        pltpu.VMEM((2 * y_size, tok, 2 * HD), jnp.bfloat16),
    ]
    work = 2 * y_size * rows * BK * HD * 16
    across = from_across(half)
    other_query = shifted(query, "sp_2", 1)
    (closest,) = call(
        own_plane_kernel,
        [((2, rows, HD), jnp.float32)],
        (at, query, other_query, half, across),
        scratch,
        work // 2,
    )
    state = ()
    for k in range(1, z_size // 2 + 1):
        last = k == z_size // 2
        if k == 3:
            half, closest = lax.optimization_barrier((half, closest))
        if k == 4:
            half, before = lax.optimization_barrier((half, before))
        half = counter_shifted(half)
        across = from_across(half)
        state = call(
            functools.partial(plane_kernel, k, z_size, k == 1, last),
            [((3, rows, HD), jnp.float32), ((2, rows, HD), jnp.float32)]
            if last
            else [((2, 2 * rows, HD), jnp.float32)],
            (at, query, other_query, half, across) + state + ((closest,) if last else ()),
            scratch,
            work * 2,
        )
        state = tuple(state)
        if k == 1:
            before = state[0]
    mine, theirs = state
    return call(
        merge_kernel,
        [((tok, query.shape[1]), jnp.bfloat16)],
        (at, mine, shifted(theirs, "sp_2", 1)),
    )[0]


def chosen_slots(slots, weights, count):
    slot = lax.broadcasted_iota(jnp.int32, (slots.shape[0], count), 1)
    picked = jnp.zeros(slot.shape, jnp.float32)
    for k in range(slots.shape[1]):
        picked += jnp.where(slot == slots[:, k : k + 1], weights[:, k : k + 1], 0.0)
    return picked


def project_kernel(
    at_ref, heads_ref, w0, w1, far0, far1, w3, stream_ref, gain_ref, slots_ref, mid_ref, normed_ref, out_ref
):
    own, count = at_ref[3], heads_ref.shape[0]
    attended = jnp.zeros(stream_ref.shape, jnp.float32)
    for k, weight in ((0, w0), (1, w1), (3, w3)):
        heads = heads_ref[(own + count - k) % count]
        attended += jnp.dot(heads, weight[...], preferred_element_type=jnp.float32)
    heads = heads_ref[(own + count - 2) % count]
    half = far0.shape[0]
    attended += jnp.dot(heads[:, :half], far0[...], preferred_element_type=jnp.float32)
    attended += jnp.dot(heads[:, half:], far1[...], preferred_element_type=jnp.float32)
    mid = (stream_ref[...].astype(jnp.float32) + attended).astype(jnp.bfloat16)
    mid_ref[...] = mid
    wide = mid.astype(jnp.float32)
    scale = lax.rsqrt(jnp.mean(wide * wide, axis=1, keepdims=True) + 1e-06)
    normed = (wide * scale * gain_ref[...]).astype(jnp.bfloat16)
    normed_ref[...] = normed
    ones = jnp.ones(slots_ref.shape, jnp.float32)
    picked = chosen_slots(slots_ref[...], ones, out_ref.shape[0]).astype(jnp.bfloat16)
    out_ref[...] = lax.dot_general(
        picked, normed, (((0,), (0,)), ((), ())), preferred_element_type=jnp.float32
    ).astype(jnp.bfloat16)


def gated(rows, gate, up):
    gate_part = jnp.dot(rows, gate, preferred_element_type=jnp.float32)
    up_part = jnp.dot(rows, up, preferred_element_type=jnp.float32)
    return (gate_part / (1.0 + jnp.exp(-gate_part)) * up_part).astype(jnp.bfloat16)


def expert_kernel(at_ref, rows_ref, gate_ref, up_ref, down_ref, out_ref):
    chunk = 256

    def part(k, _):
        here = pl.ds(pl.multiple_of(k * chunk, chunk), chunk)
        hidden = gated(rows_ref[here, :], gate_ref[...], up_ref[...])
        out_ref[here, :] = jnp.dot(
            hidden, down_ref[...], preferred_element_type=jnp.float32
        ).astype(jnp.bfloat16)
        return 0

    lax.fori_loop(0, rows_ref.shape[0] // chunk, part, 0)


def shared_kernel(at_ref, normed_ref, mid_ref, gate_ref, up_ref, down_ref, base_ref):
    hidden = gated(normed_ref[...], gate_ref[...], up_ref[...])
    base_ref[...] = mid_ref[...].astype(jnp.float32) + jnp.dot(
        hidden, down_ref[...], preferred_element_type=jnp.float32
    )


def combine_kernel(at_ref, base_ref, rows_ref, slots_ref, weights_ref, out_ref):
    picked = chosen_slots(slots_ref[...], weights_ref[...], rows_ref.shape[0])
    high = picked.astype(jnp.bfloat16)
    low = (picked - high.astype(jnp.float32)).astype(jnp.bfloat16)
    routed = jnp.dot(high, rows_ref[...], preferred_element_type=jnp.float32)
    routed += jnp.dot(low, rows_ref[...], preferred_element_type=jnp.float32)
    out_ref[...] = (base_ref[...] + routed).astype(jnp.bfloat16)


def per_device(
    query,
    key_rows,
    value_rows,
    stream,
    out_weight,
    norm_gain,
    route_ids,
    route_weights,
    expert_gate,
    expert_up,
    expert_down,
    shared_gate,
    shared_up,
    shared_down,
):
    at = jnp.stack([lax.axis_index(axis) for axis in SP_TP])
    weight_below = shifted(out_weight, "tp", 1)
    weight_above = shifted(out_weight, "tp", -1)
    half = out_weight.shape[0] // 2
    far0 = shifted(weight_below[:half], "tp", 1)
    far1 = shifted(weight_above[half:], "tp", -1)
    out_weights = (out_weight, weight_below, far0, far1, weight_above)
    own_rows = stream.shape[0]
    expert_count = lax.axis_size(SP) * expert_gate.shape[0]
    capacity = 2 * own_rows * TOP_K // expert_count
    slot_count = expert_count * capacity
    flat_ids = route_ids.reshape(-1)
    membership = (flat_ids[:, None] == jnp.arange(expert_count, dtype=jnp.int32)[None, :]).astype(
        jnp.int32
    )
    before = jnp.cumsum(membership, axis=0) - membership
    slot_rank = jnp.sum(before * membership, axis=1)
    slots = (flat_ids * capacity + slot_rank).reshape(route_ids.shape)
    heads_out = attention(at, query, key_rows, value_rows)
    token_heads = lax.all_to_all(
        heads_out.reshape(-1, own_rows, heads_out.shape[1]), "tp", 0, 0, tiled=True
    )
    wide = (own_rows, D)
    mid, normed, outgoing = call(
        project_kernel,
        [(wide, jnp.bfloat16), (wide, jnp.bfloat16), ((slot_count, D), jnp.bfloat16)],
        (at, token_heads, *out_weights, stream, norm_gain.reshape(1, D), slots),
        flops=2**29,
    )
    exchange = (lax.axis_size(SP), slot_count // lax.axis_size(SP), D)
    arrived = lax.all_to_all(outgoing.reshape(exchange), SP, 0, 0, tiled=True)
    (produced,) = call(
        expert_kernel,
        [((slot_count, D), jnp.bfloat16)],
        (at, arrived.reshape(slot_count, D), expert_gate[0], expert_up[0], expert_down[0]),
        flops=2**32,
    )
    returned = lax.all_to_all(produced.reshape(exchange), SP, 0, 0, tiled=True)
    (base,) = call(
        shared_kernel,
        [(wide, jnp.float32)],
        (at, normed, mid, shared_gate, shared_up, shared_down),
        flops=2**30,
    )
    return call(
        combine_kernel,
        [(wide, jnp.bfloat16)],
        (at, base, returned.reshape(slot_count, D), slots, route_weights),
        flops=2**28,
    )[0]


def solution(mesh):
    split = Mesh(mesh.devices.reshape(8, 4, 2, mesh.shape["tp"]), ("sp_0", "sp_1", "sp_2", "tp"))
    in_specs = (
        P(SP, "tp"),
        P(SP, "tp"),
        P(SP, "tp"),
        P(SP_TP, None),
        P("tp", None),
        P(),
        P(SP_TP, None),
        P(SP_TP, None),
        P(SP, None, None),
        P(SP, None, None),
        P(SP, None, None),
        P(),
        P(),
        P(),
    )
    out_specs = P(SP_TP, None)

    return jax.shard_map(
        per_device, mesh=split, in_specs=in_specs, out_specs=out_specs, check_vma=False
    )
```

```python
import functools
import math

import jax
import jax.numpy as jnp
from jax import lax
from jax.experimental import pallas as pl
from jax.experimental.pallas import tpu as pltpu
from jax.sharding import Mesh
from jax.sharding import PartitionSpec as P


D = 2048
HD = 128
TOP_K = 4
SP = ("sp_0", "sp_1", "sp_2")
SP_TP = ("sp_0", "sp_1", "sp_2", "tp")


BK = 256
SCALE = math.log2(math.e) / math.sqrt(HD)


def shifted(value, axis, step):
    size = lax.axis_size(axis)
    return lax.ppermute(value, axis, [(i, (i + step) % size) for i in range(size)])


def counter_shifted(value):
    size = lax.axis_size("sp_0")
    pairs = [(2 * i, 2 * ((i + 1) % size)) for i in range(size)]
    pairs += [(2 * i + 1, 2 * ((i - 1) % size) + 1) for i in range(size)]
    return lax.ppermute(value, ("sp_0", "sp_2"), pairs)


def call(kernel, outs, args, scratch=(), flops=0):
    near = pl.BlockSpec(memory_space=pltpu.VMEM)
    return pl.pallas_call(
        kernel,
        out_shape=[jax.ShapeDtypeStruct(*out) for out in outs],
        in_specs=[pl.BlockSpec(memory_space=pltpu.SMEM)]
        + [near] * (len(args) - 1),
        out_specs=[near] * len(outs),
        scratch_shapes=list(scratch),
        compiler_params=pltpu.CompilerParams(vmem_limit_bytes=24 * 2**20),
        cost_estimate=pl.CostEstimate(flops=flops, bytes_accessed=2**20, transcendentals=0),
    )(*args)


def assemble_kernel(at_ref, own_ref, other_ref, part_ref):
    core = at_ref[2]
    for k in range(own_ref.shape[0]):
        part_ref[2 * k + core] = own_ref[k]
        part_ref[2 * k + 1 - core] = other_ref[k]


def join_plane(at_ref, part_ref, before_ref, after_ref, plane):
    count = plane.shape[0] // 2
    sources = ((0, part_ref, 0), (1, part_ref, 2), (2, after_ref, 0), (3, before_ref, 0))
    for ahead, ref, first in sources:
        place = 2 * ((at_ref[1] + ahead) % count)
        for core in range(2):
            plane[place + core] = ref[first + core]


def block_steps(q_ref, plane_ref, acc, carry, tri, level_buf, penalty_buf, first_row, tok, base=0):
    rows = acc.shape[0]

    def scores(j, slot, diagonal=False):
        keys = plane_ref[base + j, :, 0:HD]
        y = lax.dot_general(
            q_ref[pl.ds(first_row, rows), :],
            jnp.concatenate([keys, keys], axis=1),
            (((1,), (1,)), ((), ())),
            preferred_element_type=jnp.float32,
        )
        penalty = jnp.maximum(y, jnp.log2(1.0 + jnp.exp2(jnp.minimum(y, 126.0))))
        level = y - penalty
        if diagonal:
            query_at = lax.broadcasted_iota(jnp.int32, (rows, BK), 0) % tok
            visible = lax.broadcasted_iota(jnp.int32, (rows, BK), 1) < query_at
            penalty = jnp.where(visible, penalty, 0.0)
            level = jnp.where(visible, level, -1e30)
        level_buf[slot] = level
        penalty_buf[slot] = penalty.astype(jnp.bfloat16)

    def mix(j, slot):
        penalty = penalty_buf[slot]
        after = jnp.dot(penalty, tri[...], preferred_element_type=jnp.float32)
        so_far = carry[...]
        weights = jnp.exp2(level_buf[slot] - after - jnp.concatenate([so_far, so_far], axis=1))
        carry[...] = so_far + jnp.broadcast_to(
            after[:, 0:1] + penalty[:, 0:1].astype(jnp.float32), (rows, HD)
        )
        acc[...] += jnp.dot(
            weights.astype(jnp.bfloat16),
            plane_ref[base + j, :, HD : 2 * HD],
            preferred_element_type=jnp.float32,
        )

    def both(j, slot):
        mix(j, slot)
        scores(j - 1, 1 - slot)

    return scores, mix, both


def clear(acc, carry, tri):
    acc[...] = jnp.zeros_like(acc)
    carry[...] = jnp.zeros_like(carry)
    key_at = lax.broadcasted_iota(jnp.int32, (BK, BK), 0)
    later = key_at > lax.broadcasted_iota(jnp.int32, (BK, BK), 1)
    tri[...] = later.astype(jnp.float32).astype(jnp.bfloat16)


def scale_queries(at_ref, own_ref, other_ref, q_ref):
    tok = own_ref.shape[0]
    heads = own_ref.shape[1] // HD
    core = at_ref[2]
    for place, ref in ((core, own_ref), (1 - core, other_ref)):
        for g in range(heads):
            scaled = ref[:, g * HD : (g + 1) * HD].astype(jnp.float32) * SCALE
            high = scaled.astype(jnp.bfloat16)
            target = pl.ds(pl.multiple_of(place * tok * heads + g * tok, tok), tok)
            q_ref[target, 0:HD] = high
            q_ref[target, HD : 2 * HD] = (scaled - high.astype(jnp.float32)).astype(jnp.bfloat16)


def own_plane_kernel(
    at_ref, own_ref, other_ref, part_ref, before_ref, after_ref, out_ref,
    q_buf, acc, carry, tri, level_buf, penalty_buf, plane,
):
    rows = acc.shape[0]
    core = at_ref[2]
    scale_queries(at_ref, own_ref, other_ref, q_buf)
    clear(acc, carry, tri)
    join_plane(at_ref, part_ref, before_ref, after_ref, plane)
    first_row = pl.multiple_of(core * rows, rows)
    scores, mix, both = block_steps(
        q_buf, plane, acc, carry, tri, level_buf, penalty_buf, first_row, own_ref.shape[0]
    )
    pos = 2 * at_ref[1] + core
    scores(pos, 0, diagonal=True)

    def step(i, _):
        both(pos - 2 * i, 0)
        both(pos - 2 * i - 1, 1)
        return 0

    lax.fori_loop(0, pos // 2, step, 0)

    @pl.when(pos % 2 == 1)
    def _():
        both(1, 0)
        mix(0, 1)

    @pl.when(pos % 2 == 0)
    def _():
        mix(0, 0)

    out_ref[0] = acc[...]
    out_ref[1] = carry[...]


def plane_kernel(distance, z_size, first, last, at_ref, own_ref, other_ref, *refs):
    part_ref, before_ref, after_ref, *refs = refs
    if not first:
        state, *refs = refs
    if last:
        closest, mine_ref, theirs_ref, *refs = refs
    else:
        out_ref, *refs = refs
    q_buf, acc, carry, tri, level_buf, penalty_buf, plane = refs
    rows = acc.shape[0]
    core = at_ref[2]
    below = jnp.where(core == 0, distance, z_size - distance)
    visible = below <= at_ref[0]
    shards = plane.shape[0] // 2 if last else plane.shape[0]
    upward = core == 0
    base = shards * (1 - core) if last else 0

    @pl.when(visible)
    def _():
        scale_queries(at_ref, own_ref, other_ref, q_buf)
        join_plane(at_ref, part_ref, before_ref, after_ref, plane)

    def part(turn, _):
        first_row = pl.multiple_of(jnp.where(turn == 0, 1 - core, core) * rows, rows)
        here = pl.ds(first_row, rows)
        clear(acc, carry, tri)

        @pl.when(visible)
        def _():
            scores, mix, both = block_steps(
                q_buf, plane, acc, carry, tri, level_buf, penalty_buf, first_row,
                own_ref.shape[0], base,
            )
            scores(shards - 1, 0)

            def step(i, _):
                both(shards - 1 - 2 * i, 0)
                both(shards - 2 - 2 * i, 1)
                return 0

            lax.fori_loop(0, shards // 2 - 1, step, 0)
            both(1, 0)
            mix(0, 1)

        result, total = acc[...], carry[...]
        if not first:
            old, old_total = state[0, here, :], state[1, here, :]
            result = result * jnp.exp2(jnp.where(upward, -old_total, 0.0))
            result = result + old * jnp.exp2(jnp.where(upward, 0.0, -total))
            total = total + old_total
        if not last:
            out_ref[0, here, :] = result
            out_ref[1, here, :] = total
            return 0

        @pl.when(turn == 0)
        def _():
            theirs_ref[0] = result
            theirs_ref[1] = total

        @pl.when(turn == 1)
        def _():
            left = jnp.exp2(-closest[1])
            mine_ref[0] = closest[0] + jnp.where(upward, left * result, 0.0)
            mine_ref[1] = jnp.where(upward, left * jnp.exp2(-total), left)
            mine_ref[2] = jnp.where(upward, 0.0, left * result)

        return 0

    lax.fori_loop(0, 2, part, 0)


def merge_kernel(at_ref, mine, theirs, out_ref):
    upward = at_ref[2] == 0
    tok = out_ref.shape[0]
    older = jnp.where(upward, 0.0, jnp.exp2(-theirs[1])) * mine[2]
    mixed = mine[0] + mine[1] * theirs[0] + older
    for g in range(out_ref.shape[1] // HD):
        out_ref[:, g * HD : (g + 1) * HD] = mixed[g * tok : (g + 1) * tok].astype(out_ref.dtype)


def attention(at, query, keys, values):
    z_size, y_size = lax.axis_size("sp_0"), lax.axis_size("sp_1")
    tok = query.shape[0]
    rows = tok * (query.shape[1] // HD)
    pair = jnp.concatenate([keys, values], axis=1)
    own_rows = jnp.stack([pair, shifted(pair, "sp_1", -1)])
    (part,) = call(
        assemble_kernel,
        [((y_size, tok, 2 * HD), jnp.bfloat16)],
        (at, own_rows, shifted(own_rows, "sp_2", 1)),
    )

    def from_neighbours(value):
        before = shifted(value[:2], "sp_1", 1)
        after = shifted(value[2:], "sp_1", -1)
        return value, before, after

    scratch = [
        pltpu.VMEM((2 * rows, 2 * HD), jnp.bfloat16),
        pltpu.VMEM((rows, HD), jnp.float32),
        pltpu.VMEM((rows, HD), jnp.float32),
        pltpu.VMEM((BK, BK), jnp.bfloat16),
        pltpu.VMEM((2, rows, BK), jnp.float32),
        pltpu.VMEM((2, rows, BK), jnp.bfloat16),
        pltpu.VMEM((2 * y_size, tok, 2 * HD), jnp.bfloat16),
    ]
    work = 2 * y_size * rows * BK * HD * 16
    held = from_neighbours(part)
    other_query = shifted(query, "sp_2", 1)
    (closest,) = call(
        own_plane_kernel,
        [((2, rows, HD), jnp.float32)],
        (at, query, other_query, *held),
        scratch,
        work // 2,
    )
    state = ()
    for k in range(1, z_size // 2 + 1):
        last = k == z_size // 2
        if k == 3:
            part, closest = lax.optimization_barrier((part, closest))
        if k == 4:
            part, early = lax.optimization_barrier((part, early))
        part = counter_shifted(part)
        held = from_neighbours(part)
        state = call(
            functools.partial(plane_kernel, k, z_size, k == 1, last),
            [((3, rows, HD), jnp.float32), ((2, rows, HD), jnp.float32)]
            if last
            else [((2, 2 * rows, HD), jnp.float32)],
            (at, query, other_query, *held) + state + ((closest,) if last else ()),
            scratch,
            work * 2,
        )
        state = tuple(state)
        if k == 1:
            early = state[0]
    mine, theirs = state
    return call(
        merge_kernel,
        [((tok, query.shape[1]), jnp.bfloat16)],
        (at, mine, shifted(theirs, "sp_2", 1)),
    )[0]


def chosen_slots(slots, weights, count):
    slot = lax.broadcasted_iota(jnp.int32, (slots.shape[0], count), 1)
    picked = jnp.zeros(slot.shape, jnp.float32)
    for k in range(slots.shape[1]):
        picked += jnp.where(slot == slots[:, k : k + 1], weights[:, k : k + 1], 0.0)
    return picked


def project_kernel(
    at_ref, heads_ref, w0, w1, far0, far1, w3, stream_ref, gain_ref, slots_ref, mid_ref, normed_ref, out_ref
):
    own, count = at_ref[3], heads_ref.shape[0]
    attended = jnp.zeros(stream_ref.shape, jnp.float32)
    for k, weight in ((0, w0), (1, w1), (3, w3)):
        heads = heads_ref[(own + count - k) % count]
        attended += jnp.dot(heads, weight[...], preferred_element_type=jnp.float32)
    heads = heads_ref[(own + count - 2) % count]
    half = far0.shape[0]
    attended += jnp.dot(heads[:, :half], far0[...], preferred_element_type=jnp.float32)
    attended += jnp.dot(heads[:, half:], far1[...], preferred_element_type=jnp.float32)
    mid = (stream_ref[...].astype(jnp.float32) + attended).astype(jnp.bfloat16)
    mid_ref[...] = mid
    wide = mid.astype(jnp.float32)
    scale = lax.rsqrt(jnp.mean(wide * wide, axis=1, keepdims=True) + 1e-06)
    normed = (wide * scale * gain_ref[...]).astype(jnp.bfloat16)
    normed_ref[...] = normed
    ones = jnp.ones(slots_ref.shape, jnp.float32)
    picked = chosen_slots(slots_ref[...], ones, out_ref.shape[0]).astype(jnp.bfloat16)
    out_ref[...] = lax.dot_general(
        picked, normed, (((0,), (0,)), ((), ())), preferred_element_type=jnp.float32
    ).astype(jnp.bfloat16)


def gated(rows, gate, up):
    gate_part = jnp.dot(rows, gate, preferred_element_type=jnp.float32)
    up_part = jnp.dot(rows, up, preferred_element_type=jnp.float32)
    return (gate_part / (1.0 + jnp.exp(-gate_part)) * up_part).astype(jnp.bfloat16)


def expert_kernel(at_ref, rows_ref, gate_ref, up_ref, down_ref, out_ref):
    chunk = 256

    def part(k, _):
        here = pl.ds(pl.multiple_of(k * chunk, chunk), chunk)
        hidden = gated(rows_ref[here, :], gate_ref[...], up_ref[...])
        out_ref[here, :] = jnp.dot(
            hidden, down_ref[...], preferred_element_type=jnp.float32
        ).astype(jnp.bfloat16)
        return 0

    lax.fori_loop(0, rows_ref.shape[0] // chunk, part, 0)


def shared_kernel(at_ref, normed_ref, mid_ref, gate_ref, up_ref, down_ref, base_ref):
    hidden = gated(normed_ref[...], gate_ref[...], up_ref[...])
    base_ref[...] = mid_ref[...].astype(jnp.float32) + jnp.dot(
        hidden, down_ref[...], preferred_element_type=jnp.float32
    )


def combine_kernel(at_ref, base_ref, rows_ref, slots_ref, weights_ref, out_ref):
    picked = chosen_slots(slots_ref[...], weights_ref[...], rows_ref.shape[0])
    high = picked.astype(jnp.bfloat16)
    low = (picked - high.astype(jnp.float32)).astype(jnp.bfloat16)
    routed = jnp.dot(high, rows_ref[...], preferred_element_type=jnp.float32)
    routed += jnp.dot(low, rows_ref[...], preferred_element_type=jnp.float32)
    out_ref[...] = (base_ref[...] + routed).astype(jnp.bfloat16)


def per_device(
    query,
    key_rows,
    value_rows,
    stream,
    out_weight,
    norm_gain,
    route_ids,
    route_weights,
    expert_gate,
    expert_up,
    expert_down,
    shared_gate,
    shared_up,
    shared_down,
):
    at = jnp.stack([lax.axis_index(axis) for axis in SP_TP])
    weight_below = shifted(out_weight, "tp", 1)
    weight_above = shifted(out_weight, "tp", -1)
    half = out_weight.shape[0] // 2
    far0 = shifted(weight_below[:half], "tp", 1)
    far1 = shifted(weight_above[half:], "tp", -1)
    out_weights = (out_weight, weight_below, far0, far1, weight_above)
    own_rows = stream.shape[0]
    expert_count = lax.axis_size(SP) * expert_gate.shape[0]
    capacity = 2 * own_rows * TOP_K // expert_count
    slot_count = expert_count * capacity
    flat_ids = route_ids.reshape(-1)
    membership = (flat_ids[:, None] == jnp.arange(expert_count, dtype=jnp.int32)[None, :]).astype(
        jnp.int32
    )
    before = jnp.cumsum(membership, axis=0) - membership
    slot_rank = jnp.sum(before * membership, axis=1)
    slots = (flat_ids * capacity + slot_rank).reshape(route_ids.shape)
    heads_out = attention(at, query, key_rows, value_rows)
    token_heads = lax.all_to_all(
        heads_out.reshape(-1, own_rows, heads_out.shape[1]), "tp", 0, 0, tiled=True
    )
    wide = (own_rows, D)
    mid, normed, outgoing = call(
        project_kernel,
        [(wide, jnp.bfloat16), (wide, jnp.bfloat16), ((slot_count, D), jnp.bfloat16)],
        (at, token_heads, *out_weights, stream, norm_gain.reshape(1, D), slots),
        flops=2**29,
    )
    exchange = (lax.axis_size(SP), slot_count // lax.axis_size(SP), D)
    arrived = lax.all_to_all(outgoing.reshape(exchange), SP, 0, 0, tiled=True)
    (produced,) = call(
        expert_kernel,
        [((slot_count, D), jnp.bfloat16)],
        (at, arrived.reshape(slot_count, D), expert_gate[0], expert_up[0], expert_down[0]),
        flops=2**32,
    )
    returned = lax.all_to_all(produced.reshape(exchange), SP, 0, 0, tiled=True)
    (base,) = call(
        shared_kernel,
        [(wide, jnp.float32)],
        (at, normed, mid, shared_gate, shared_up, shared_down),
        flops=2**30,
    )
    return call(
        combine_kernel,
        [(wide, jnp.bfloat16)],
        (at, base, returned.reshape(slot_count, D), slots, route_weights),
        flops=2**28,
    )[0]


def solution(mesh):
    split = Mesh(mesh.devices.reshape(8, 4, 2, mesh.shape["tp"]), ("sp_0", "sp_1", "sp_2", "tp"))
    in_specs = (
        P(SP, "tp"),
        P(SP, "tp"),
        P(SP, "tp"),
        P(SP_TP, None),
        P("tp", None),
        P(),
        P(SP_TP, None),
        P(SP_TP, None),
        P(SP, None, None),
        P(SP, None, None),
        P(SP, None, None),
        P(),
        P(),
        P(),
    )
    out_specs = P(SP_TP, None)

    return jax.shard_map(
        per_device, mesh=split, in_specs=in_specs, out_specs=out_specs, check_vma=False
    )
```

```python
import functools
import math

import jax
import jax.numpy as jnp
from jax import lax
from jax.experimental import pallas as pl
from jax.experimental.pallas import tpu as pltpu
from jax.sharding import Mesh
from jax.sharding import PartitionSpec as P


D = 2048
HD = 128
TOP_K = 4
SP = ("sp_0", "sp_1", "sp_2")
SP_TP = ("sp_0", "sp_1", "sp_2", "tp")


BK = 256
SCALE = math.log2(math.e) / math.sqrt(HD)


def shifted(value, axis, step):
    size = lax.axis_size(axis)
    return lax.ppermute(value, axis, [(i, (i + step) % size) for i in range(size)])


def counter_shifted(value):
    size = lax.axis_size("sp_0")
    pairs = [(2 * i, 2 * ((i + 1) % size)) for i in range(size)]
    pairs += [(2 * i + 1, 2 * ((i - 1) % size) + 1) for i in range(size)]
    return lax.ppermute(value, ("sp_0", "sp_2"), pairs)


def call(kernel, outs, args, scratch=(), flops=0):
    near = pl.BlockSpec(memory_space=pltpu.VMEM)
    return pl.pallas_call(
        kernel,
        out_shape=[jax.ShapeDtypeStruct(*out) for out in outs],
        in_specs=[pl.BlockSpec(memory_space=pltpu.SMEM)]
        + [near] * (len(args) - 1),
        out_specs=[near] * len(outs),
        scratch_shapes=list(scratch),
        compiler_params=pltpu.CompilerParams(vmem_limit_bytes=24 * 2**20),
        cost_estimate=pl.CostEstimate(flops=flops, bytes_accessed=2**20, transcendentals=0),
    )(*args)


def assemble_kernel(at_ref, own_ref, other_ref, part_ref):
    core = at_ref[2]
    for k in range(own_ref.shape[0]):
        part_ref[2 * k + core] = own_ref[k]
        part_ref[2 * k + 1 - core] = other_ref[k]


def join_plane(at_ref, part_ref, before_ref, after_ref, plane):
    count = plane.shape[0] // 2
    sources = ((0, part_ref, 0), (1, part_ref, 2), (2, after_ref, 0), (3, before_ref, 0))
    for ahead, ref, first in sources:
        place = 2 * ((at_ref[1] + ahead) % count)
        for core in range(2):
            plane[place + core] = ref[first + core]


def block_steps(q_ref, plane_ref, acc, carry, tri, level_buf, penalty_buf, tok, base=0):
    rows = level_buf.shape[1]

    def scores(first_row, j, slot, diagonal=False):
        keys = plane_ref[base + j, :, 0:HD]
        y = lax.dot_general(
            q_ref[pl.ds(first_row, rows), :],
            jnp.concatenate([keys, keys], axis=1),
            (((1,), (1,)), ((), ())),
            preferred_element_type=jnp.float32,
        )
        penalty = jnp.maximum(y, jnp.log2(1.0 + jnp.exp2(jnp.minimum(y, 126.0))))
        level = y - penalty
        if diagonal:
            query_at = lax.broadcasted_iota(jnp.int32, (rows, BK), 0) % tok
            visible = lax.broadcasted_iota(jnp.int32, (rows, BK), 1) < query_at
            penalty = jnp.where(visible, penalty, 0.0)
            level = jnp.where(visible, level, -1e30)
        level_buf[slot] = level
        penalty_buf[slot] = penalty.astype(jnp.bfloat16)

    def mix(first_row, j, slot):
        here = pl.ds(first_row, rows)
        penalty = penalty_buf[slot]
        after = jnp.dot(penalty, tri[...], preferred_element_type=jnp.float32)
        so_far = carry[here, :]
        weights = jnp.exp2(level_buf[slot] - after - jnp.concatenate([so_far, so_far], axis=1))
        carry[here, :] = so_far + jnp.broadcast_to(
            after[:, 0:1] + penalty[:, 0:1].astype(jnp.float32), (rows, HD)
        )
        acc[here, :] += jnp.dot(
            weights.astype(jnp.bfloat16),
            plane_ref[base + j, :, HD : 2 * HD],
            preferred_element_type=jnp.float32,
        )

    return scores, mix


def clear(acc, carry, tri):
    acc[...] = jnp.zeros_like(acc)
    carry[...] = jnp.zeros_like(carry)
    key_at = lax.broadcasted_iota(jnp.int32, (BK, BK), 0)
    later = key_at > lax.broadcasted_iota(jnp.int32, (BK, BK), 1)
    tri[...] = later.astype(jnp.float32).astype(jnp.bfloat16)


def scale_queries(at_ref, own_ref, other_ref, q_ref):
    tok = own_ref.shape[0]
    heads = own_ref.shape[1] // HD
    core = at_ref[2]
    for place, ref in ((core, own_ref), (1 - core, other_ref)):
        for g in range(heads):
            scaled = ref[:, g * HD : (g + 1) * HD].astype(jnp.float32) * SCALE
            high = scaled.astype(jnp.bfloat16)
            target = pl.ds(pl.multiple_of(place * tok * heads + g * tok, tok), tok)
            q_ref[target, 0:HD] = high
            q_ref[target, HD : 2 * HD] = (scaled - high.astype(jnp.float32)).astype(jnp.bfloat16)


def own_plane_kernel(
    at_ref, own_ref, other_ref, part_ref, before_ref, after_ref, out_ref,
    q_buf, acc, carry, tri, level_buf, penalty_buf, plane,
):
    rows = acc.shape[0]
    core = at_ref[2]
    scale_queries(at_ref, own_ref, other_ref, q_buf)
    clear(acc, carry, tri)
    join_plane(at_ref, part_ref, before_ref, after_ref, plane)
    first_row = pl.multiple_of(core * rows, rows)
    scores, mix = block_steps(
        q_buf, plane, acc, carry, tri, level_buf, penalty_buf, own_ref.shape[0]
    )
    pos = 2 * at_ref[1] + core
    scores(first_row, pos, 0, diagonal=True)

    def both(j, slot):
        mix(0, j, slot)
        scores(first_row, j - 1, 1 - slot)

    def step(i, _):
        both(pos - 2 * i, 0)
        both(pos - 2 * i - 1, 1)
        return 0

    lax.fori_loop(0, pos // 2, step, 0)

    @pl.when(pos % 2 == 1)
    def _():
        both(1, 0)
        mix(0, 0, 1)

    @pl.when(pos % 2 == 0)
    def _():
        mix(0, 0, 0)

    out_ref[0] = acc[...]
    out_ref[1] = carry[...]


def plane_kernel(distance, z_size, first, last, at_ref, own_ref, other_ref, *refs):
    part_ref, before_ref, after_ref, *refs = refs
    if not first:
        state, *refs = refs
    if last:
        closest, mine_ref, theirs_ref, *refs = refs
    else:
        out_ref, *refs = refs
    q_buf, acc, carry, tri, level_buf, penalty_buf, plane = refs
    rows = level_buf.shape[1]
    core = at_ref[2]
    below = jnp.where(core == 0, distance, z_size - distance)
    visible = below <= at_ref[0]
    shards = plane.shape[0] // 2 if last else plane.shape[0]
    upward = core == 0
    base = shards * (1 - core) if last else 0

    clear(acc, carry, tri)

    @pl.when(visible)
    def _():
        scale_queries(at_ref, own_ref, other_ref, q_buf)
        join_plane(at_ref, part_ref, before_ref, after_ref, plane)
        scores, mix = block_steps(
            q_buf, plane, acc, carry, tri, level_buf, penalty_buf, own_ref.shape[0], base
        )

        def unit(u):
            return pl.multiple_of(u // shards * rows, rows), shards - 1 - u % shards

        def step(i, _):
            for slot in range(2):
                mix(*unit(2 * i + slot), slot)
                scores(*unit(jnp.minimum(2 * i + slot + 1, 2 * shards - 1)), 1 - slot)
            return 0

        scores(*unit(jnp.int32(0)), 0)
        lax.fori_loop(0, shards, step, 0)

    def part(turn, _):
        first_row = pl.multiple_of(jnp.where(turn == 0, 1 - core, core) * rows, rows)
        here = pl.ds(first_row, rows)
        result, total = acc[here, :], carry[here, :]
        if not first:
            old, old_total = state[0, here, :], state[1, here, :]
            result = result * jnp.exp2(jnp.where(upward, -old_total, 0.0))
            result = result + old * jnp.exp2(jnp.where(upward, 0.0, -total))
            total = total + old_total
        if not last:
            out_ref[0, here, :] = result
            out_ref[1, here, :] = total
            return 0

        @pl.when(turn == 0)
        def _():
            theirs_ref[0] = result
            theirs_ref[1] = total

        @pl.when(turn == 1)
        def _():
            left = jnp.exp2(-closest[1])
            mine_ref[0] = closest[0] + jnp.where(upward, left * result, 0.0)
            mine_ref[1] = jnp.where(upward, left * jnp.exp2(-total), left)
            mine_ref[2] = jnp.where(upward, 0.0, left * result)

        return 0

    lax.fori_loop(0, 2, part, 0)


def merge_kernel(at_ref, mine, theirs, out_ref):
    upward = at_ref[2] == 0
    tok = out_ref.shape[0]
    older = jnp.where(upward, 0.0, jnp.exp2(-theirs[1])) * mine[2]
    mixed = mine[0] + mine[1] * theirs[0] + older
    for g in range(out_ref.shape[1] // HD):
        out_ref[:, g * HD : (g + 1) * HD] = mixed[g * tok : (g + 1) * tok].astype(out_ref.dtype)


def attention(at, query, keys, values):
    z_size, y_size = lax.axis_size("sp_0"), lax.axis_size("sp_1")
    tok = query.shape[0]
    rows = tok * (query.shape[1] // HD)
    pair = jnp.concatenate([keys, values], axis=1)
    own_rows = jnp.stack([pair, shifted(pair, "sp_1", -1)])
    (part,) = call(
        assemble_kernel,
        [((y_size, tok, 2 * HD), jnp.bfloat16)],
        (at, own_rows, shifted(own_rows, "sp_2", 1)),
    )

    def from_neighbours(value):
        before = shifted(value[:2], "sp_1", 1)
        after = shifted(value[2:], "sp_1", -1)
        return value, before, after

    def scratch(state_rows):
        return [
            pltpu.VMEM((2 * rows, 2 * HD), jnp.bfloat16),
            pltpu.VMEM((state_rows, HD), jnp.float32),
            pltpu.VMEM((state_rows, HD), jnp.float32),
            pltpu.VMEM((BK, BK), jnp.bfloat16),
            pltpu.VMEM((2, rows, BK), jnp.float32),
            pltpu.VMEM((2, rows, BK), jnp.bfloat16),
            pltpu.VMEM((2 * y_size, tok, 2 * HD), jnp.bfloat16),
        ]

    work = 2 * y_size * rows * BK * HD * 16
    held = from_neighbours(part)
    other_query = shifted(query, "sp_2", 1)
    (closest,) = call(
        own_plane_kernel,
        [((2, rows, HD), jnp.float32)],
        (at, query, other_query, *held),
        scratch(rows),
        work // 2,
    )
    state = ()
    for k in range(1, z_size // 2 + 1):
        last = k == z_size // 2
        if k == 3:
            part, closest = lax.optimization_barrier((part, closest))
        if k == 4:
            part, early = lax.optimization_barrier((part, early))
        part = counter_shifted(part)
        held = from_neighbours(part)
        state = call(
            functools.partial(plane_kernel, k, z_size, k == 1, last),
            [((3, rows, HD), jnp.float32), ((2, rows, HD), jnp.float32)]
            if last
            else [((2, 2 * rows, HD), jnp.float32)],
            (at, query, other_query, *held) + state + ((closest,) if last else ()),
            scratch(2 * rows),
            work * 2,
        )
        state = tuple(state)
        if k == 1:
            early = state[0]
    mine, theirs = state
    return call(
        merge_kernel,
        [((tok, query.shape[1]), jnp.bfloat16)],
        (at, mine, shifted(theirs, "sp_2", 1)),
    )[0]


def chosen_slots(slots, weights, count):
    slot = lax.broadcasted_iota(jnp.int32, (slots.shape[0], count), 1)
    picked = jnp.zeros(slot.shape, jnp.float32)
    for k in range(slots.shape[1]):
        picked += jnp.where(slot == slots[:, k : k + 1], weights[:, k : k + 1], 0.0)
    return picked


def project_kernel(
    at_ref, heads_ref, w0, w1, far0, far1, w3, stream_ref, gain_ref, slots_ref, mid_ref, normed_ref, out_ref
):
    own, count = at_ref[3], heads_ref.shape[0]
    attended = jnp.zeros(stream_ref.shape, jnp.float32)
    for k, weight in ((0, w0), (1, w1), (3, w3)):
        heads = heads_ref[(own + count - k) % count]
        attended += jnp.dot(heads, weight[...], preferred_element_type=jnp.float32)
    heads = heads_ref[(own + count - 2) % count]
    half = far0.shape[0]
    attended += jnp.dot(heads[:, :half], far0[...], preferred_element_type=jnp.float32)
    attended += jnp.dot(heads[:, half:], far1[...], preferred_element_type=jnp.float32)
    mid = (stream_ref[...].astype(jnp.float32) + attended).astype(jnp.bfloat16)
    mid_ref[...] = mid
    wide = mid.astype(jnp.float32)
    scale = lax.rsqrt(jnp.mean(wide * wide, axis=1, keepdims=True) + 1e-06)
    normed = (wide * scale * gain_ref[...]).astype(jnp.bfloat16)
    normed_ref[...] = normed
    ones = jnp.ones(slots_ref.shape, jnp.float32)
    picked = chosen_slots(slots_ref[...], ones, out_ref.shape[0]).astype(jnp.bfloat16)
    out_ref[...] = lax.dot_general(
        picked, normed, (((0,), (0,)), ((), ())), preferred_element_type=jnp.float32
    ).astype(jnp.bfloat16)


def gated(rows, gate, up):
    gate_part = jnp.dot(rows, gate, preferred_element_type=jnp.float32)
    up_part = jnp.dot(rows, up, preferred_element_type=jnp.float32)
    return (gate_part / (1.0 + jnp.exp(-gate_part)) * up_part).astype(jnp.bfloat16)


def expert_kernel(at_ref, rows_ref, gate_ref, up_ref, down_ref, out_ref):
    chunk = 256

    def part(k, _):
        here = pl.ds(pl.multiple_of(k * chunk, chunk), chunk)
        hidden = gated(rows_ref[here, :], gate_ref[...], up_ref[...])
        out_ref[here, :] = jnp.dot(
            hidden, down_ref[...], preferred_element_type=jnp.float32
        ).astype(jnp.bfloat16)
        return 0

    lax.fori_loop(0, rows_ref.shape[0] // chunk, part, 0)


def shared_kernel(at_ref, normed_ref, mid_ref, gate_ref, up_ref, down_ref, base_ref):
    hidden = gated(normed_ref[...], gate_ref[...], up_ref[...])
    base_ref[...] = mid_ref[...].astype(jnp.float32) + jnp.dot(
        hidden, down_ref[...], preferred_element_type=jnp.float32
    )


def combine_kernel(at_ref, base_ref, rows_ref, slots_ref, weights_ref, out_ref):
    picked = chosen_slots(slots_ref[...], weights_ref[...], rows_ref.shape[0])
    high = picked.astype(jnp.bfloat16)
    low = (picked - high.astype(jnp.float32)).astype(jnp.bfloat16)
    routed = jnp.dot(high, rows_ref[...], preferred_element_type=jnp.float32)
    routed += jnp.dot(low, rows_ref[...], preferred_element_type=jnp.float32)
    out_ref[...] = (base_ref[...] + routed).astype(jnp.bfloat16)


def per_device(
    query,
    key_rows,
    value_rows,
    stream,
    out_weight,
    norm_gain,
    route_ids,
    route_weights,
    expert_gate,
    expert_up,
    expert_down,
    shared_gate,
    shared_up,
    shared_down,
):
    at = jnp.stack([lax.axis_index(axis) for axis in SP_TP])
    weight_below = shifted(out_weight, "tp", 1)
    weight_above = shifted(out_weight, "tp", -1)
    half = out_weight.shape[0] // 2
    far0 = shifted(weight_below[:half], "tp", 1)
    far1 = shifted(weight_above[half:], "tp", -1)
    out_weights = (out_weight, weight_below, far0, far1, weight_above)
    own_rows = stream.shape[0]
    expert_count = lax.axis_size(SP) * expert_gate.shape[0]
    capacity = 2 * own_rows * TOP_K // expert_count
    slot_count = expert_count * capacity
    flat_ids = route_ids.reshape(-1)
    membership = (flat_ids[:, None] == jnp.arange(expert_count, dtype=jnp.int32)[None, :]).astype(
        jnp.int32
    )
    before = jnp.cumsum(membership, axis=0) - membership
    slot_rank = jnp.sum(before * membership, axis=1)
    slots = (flat_ids * capacity + slot_rank).reshape(route_ids.shape)
    heads_out = attention(at, query, key_rows, value_rows)
    token_heads = lax.all_to_all(
        heads_out.reshape(-1, own_rows, heads_out.shape[1]), "tp", 0, 0, tiled=True
    )
    wide = (own_rows, D)
    mid, normed, outgoing = call(
        project_kernel,
        [(wide, jnp.bfloat16), (wide, jnp.bfloat16), ((slot_count, D), jnp.bfloat16)],
        (at, token_heads, *out_weights, stream, norm_gain.reshape(1, D), slots),
        flops=2**29,
    )
    exchange = (lax.axis_size(SP), slot_count // lax.axis_size(SP), D)
    arrived = lax.all_to_all(outgoing.reshape(exchange), SP, 0, 0, tiled=True)
    (produced,) = call(
        expert_kernel,
        [((slot_count, D), jnp.bfloat16)],
        (at, arrived.reshape(slot_count, D), expert_gate[0], expert_up[0], expert_down[0]),
        flops=2**32,
    )
    returned = lax.all_to_all(produced.reshape(exchange), SP, 0, 0, tiled=True)
    (base,) = call(
        shared_kernel,
        [(wide, jnp.float32)],
        (at, normed, mid, shared_gate, shared_up, shared_down),
        flops=2**30,
    )
    return call(
        combine_kernel,
        [(wide, jnp.bfloat16)],
        (at, base, returned.reshape(slot_count, D), slots, route_weights),
        flops=2**28,
    )[0]


def solution(mesh):
    split = Mesh(mesh.devices.reshape(8, 4, 2, mesh.shape["tp"]), ("sp_0", "sp_1", "sp_2", "tp"))
    in_specs = (
        P(SP, "tp"),
        P(SP, "tp"),
        P(SP, "tp"),
        P(SP_TP, None),
        P("tp", None),
        P(),
        P(SP_TP, None),
        P(SP_TP, None),
        P(SP, None, None),
        P(SP, None, None),
        P(SP, None, None),
        P(),
        P(),
        P(),
    )
    out_specs = P(SP_TP, None)

    return jax.shard_map(
        per_device, mesh=split, in_specs=in_specs, out_specs=out_specs, check_vma=False
    )
```

```python
import functools
import math

import jax
import jax.numpy as jnp
from jax import lax
from jax.experimental import pallas as pl
from jax.experimental.pallas import tpu as pltpu
from jax.sharding import Mesh
from jax.sharding import PartitionSpec as P


D = 2048
HD = 128
TOP_K = 4
SP = ("sp_0", "sp_1", "sp_2")
SP_TP = ("sp_0", "sp_1", "sp_2", "tp")


BK = 256
SCALE = math.log2(math.e) / math.sqrt(HD)


def shifted(value, axis, step):
    size = lax.axis_size(axis)
    return lax.ppermute(value, axis, [(i, (i + step) % size) for i in range(size)])


def counter_shifted(value):
    size = lax.axis_size("sp_0")
    pairs = [(2 * i, 2 * ((i + 1) % size)) for i in range(size)]
    pairs += [(2 * i + 1, 2 * ((i - 1) % size) + 1) for i in range(size)]
    return lax.ppermute(value, ("sp_0", "sp_2"), pairs)


def call(kernel, outs, args, scratch=(), flops=0):
    near = pl.BlockSpec(memory_space=pltpu.VMEM)
    return pl.pallas_call(
        kernel,
        out_shape=[jax.ShapeDtypeStruct(*out) for out in outs],
        in_specs=[pl.BlockSpec(memory_space=pltpu.SMEM)]
        + [near] * (len(args) - 1),
        out_specs=[near] * len(outs),
        scratch_shapes=list(scratch),
        compiler_params=pltpu.CompilerParams(vmem_limit_bytes=24 * 2**20),
        cost_estimate=pl.CostEstimate(flops=flops, bytes_accessed=2**20, transcendentals=0),
    )(*args)


def assemble_kernel(at_ref, own_ref, other_ref, part_ref):
    core = at_ref[2]
    for k in range(own_ref.shape[0]):
        part_ref[2 * k + core] = own_ref[k]
        part_ref[2 * k + 1 - core] = other_ref[k]


def join_plane(at_ref, part_ref, before_ref, after_ref, plane):
    count = plane.shape[0] // 2
    sources = ((0, part_ref, 0), (1, part_ref, 2), (2, after_ref, 0), (3, before_ref, 0))
    for ahead, ref, first in sources:
        place = 2 * ((at_ref[1] + ahead) % count)
        for core in range(2):
            plane[place + core] = ref[first + core]


def block_steps(q_ref, plane_ref, acc, carry, tri, level_buf, penalty_buf, tok, base=0):
    rows = level_buf.shape[1]

    def scores(first_row, j, slot, diagonal=False):
        keys = plane_ref[base + j, :, 0:HD]
        y = lax.dot_general(
            q_ref[pl.ds(first_row, rows), :],
            jnp.concatenate([keys, keys], axis=1),
            (((1,), (1,)), ((), ())),
            preferred_element_type=jnp.float32,
        )
        penalty = jnp.maximum(y, jnp.log2(1.0 + jnp.exp2(jnp.minimum(y, 126.0))))
        level = y - penalty
        if diagonal:
            query_at = lax.broadcasted_iota(jnp.int32, (rows, BK), 0) % tok
            visible = lax.broadcasted_iota(jnp.int32, (rows, BK), 1) < query_at
            penalty = jnp.where(visible, penalty, 0.0)
            level = jnp.where(visible, level, -1e30)
        level_buf[slot] = level
        penalty_buf[slot] = penalty.astype(jnp.bfloat16)

    def mix(first_row, j, slot):
        here = pl.ds(first_row, rows)
        penalty = penalty_buf[slot]
        after = jnp.dot(penalty, tri[...], preferred_element_type=jnp.float32)
        so_far = carry[here, :]
        weights = jnp.exp2(level_buf[slot] - after - jnp.concatenate([so_far, so_far], axis=1))
        carry[here, :] = so_far + jnp.broadcast_to(
            after[:, 0:1] + penalty[:, 0:1].astype(jnp.float32), (rows, HD)
        )
        acc[here, :] += jnp.dot(
            weights.astype(jnp.bfloat16),
            plane_ref[base + j, :, HD : 2 * HD],
            preferred_element_type=jnp.float32,
        )

    return scores, mix


def clear(acc, carry, tri):
    acc[...] = jnp.zeros_like(acc)
    carry[...] = jnp.zeros_like(carry)
    key_at = lax.broadcasted_iota(jnp.int32, (BK, BK), 0)
    later = key_at > lax.broadcasted_iota(jnp.int32, (BK, BK), 1)
    tri[...] = later.astype(jnp.float32).astype(jnp.bfloat16)


def scale_queries(at_ref, own_ref, other_ref, q_ref):
    tok = own_ref.shape[0]
    heads = own_ref.shape[1] // HD
    core = at_ref[2]
    for place, ref in ((core, own_ref), (1 - core, other_ref)):
        for g in range(heads):
            scaled = ref[:, g * HD : (g + 1) * HD].astype(jnp.float32) * SCALE
            high = scaled.astype(jnp.bfloat16)
            target = pl.ds(pl.multiple_of(place * tok * heads + g * tok, tok), tok)
            q_ref[target, 0:HD] = high
            q_ref[target, HD : 2 * HD] = (scaled - high.astype(jnp.float32)).astype(jnp.bfloat16)


def own_plane_kernel(
    at_ref, own_ref, other_ref, part_ref, before_ref, after_ref, out_ref,
    q_buf, acc, carry, tri, level_buf, penalty_buf, plane,
):
    rows = acc.shape[0]
    core = at_ref[2]
    scale_queries(at_ref, own_ref, other_ref, q_buf)
    clear(acc, carry, tri)
    join_plane(at_ref, part_ref, before_ref, after_ref, plane)
    first_row = pl.multiple_of(core * rows, rows)
    scores, mix = block_steps(
        q_buf, plane, acc, carry, tri, level_buf, penalty_buf, own_ref.shape[0]
    )
    pos = 2 * at_ref[1] + core
    scores(first_row, pos, 0, diagonal=True)

    def both(j, slot):
        mix(0, j, slot)
        scores(first_row, j - 1, 1 - slot)

    def step(i, _):
        both(pos - 2 * i, 0)
        both(pos - 2 * i - 1, 1)
        return 0

    lax.fori_loop(0, pos // 2, step, 0)

    @pl.when(pos % 2 == 1)
    def _():
        both(1, 0)
        mix(0, 0, 1)

    @pl.when(pos % 2 == 0)
    def _():
        mix(0, 0, 0)

    out_ref[0] = acc[...]
    out_ref[1] = carry[...]


def plane_kernel(distance, z_size, first, last, at_ref, own_ref, other_ref, *refs):
    part_ref, before_ref, after_ref, *refs = refs
    if not first:
        state, *refs = refs
    if last:
        closest, mine_ref, theirs_ref, *refs = refs
    else:
        out_ref, *refs = refs
    q_buf, acc, carry, tri, level_buf, penalty_buf, plane = refs
    rows = level_buf.shape[1]
    core = at_ref[2]
    below = jnp.where(core == 0, distance, z_size - distance)
    visible = below <= at_ref[0]
    shards = plane.shape[0] // 2 if last else plane.shape[0]
    upward = core == 0
    base = shards * (1 - core) if last else 0

    clear(acc, carry, tri)

    @pl.when(visible)
    def _():
        scale_queries(at_ref, own_ref, other_ref, q_buf)
        join_plane(at_ref, part_ref, before_ref, after_ref, plane)
        scores, mix = block_steps(
            q_buf, plane, acc, carry, tri, level_buf, penalty_buf, own_ref.shape[0], base
        )

        def unit(u):
            return pl.multiple_of(u // shards * rows, rows), shards - 1 - u % shards

        def step(i, _):
            for slot in range(2):
                mix(*unit(2 * i + slot), slot)
                scores(*unit(jnp.minimum(2 * i + slot + 1, 2 * shards - 1)), 1 - slot)
            return 0

        scores(*unit(jnp.int32(0)), 0)
        lax.fori_loop(0, shards, step, 0)

    def part(turn, _):
        first_row = pl.multiple_of(jnp.where(turn == 0, 1 - core, core) * rows, rows)
        here = pl.ds(first_row, rows)
        result, total = acc[here, :], carry[here, :]
        if not first:
            old, old_total = state[0, here, :], state[1, here, :]
            result = result * jnp.exp2(jnp.where(upward, -old_total, 0.0))
            result = result + old * jnp.exp2(jnp.where(upward, 0.0, -total))
            total = total + old_total
        if not last:
            out_ref[0, here, :] = result
            out_ref[1, here, :] = total
            return 0

        @pl.when(turn == 0)
        def _():
            theirs_ref[0] = result
            theirs_ref[1] = total

        @pl.when(turn == 1)
        def _():
            left = jnp.exp2(-closest[1])
            mine_ref[0] = closest[0] + jnp.where(upward, left * result, 0.0)
            mine_ref[1] = jnp.where(upward, left * jnp.exp2(-total), left)
            mine_ref[2] = jnp.where(upward, 0.0, left * result)

        return 0

    lax.fori_loop(0, 2, part, 0)


def merge_kernel(at_ref, mine, theirs, out_ref):
    upward = at_ref[2] == 0
    tok = out_ref.shape[0]
    older = jnp.where(upward, 0.0, jnp.exp2(-theirs[1])) * mine[2]
    mixed = mine[0] + mine[1] * theirs[0] + older
    for g in range(out_ref.shape[1] // HD):
        out_ref[:, g * HD : (g + 1) * HD] = mixed[g * tok : (g + 1) * tok].astype(out_ref.dtype)


def attention(at, query, keys, values):
    z_size, y_size = lax.axis_size("sp_0"), lax.axis_size("sp_1")
    tok = query.shape[0]
    rows = tok * (query.shape[1] // HD)
    pair = jnp.concatenate([keys, values], axis=1)
    own_rows = jnp.stack([pair, shifted(pair, "sp_1", -1)])
    (part,) = call(
        assemble_kernel,
        [((y_size, tok, 2 * HD), jnp.bfloat16)],
        (at, own_rows, shifted(own_rows, "sp_2", 1)),
    )

    def from_neighbours(value):
        before = shifted(value[:2], "sp_1", 1)
        after = shifted(value[2:], "sp_1", -1)
        return value, before, after

    def scratch(state_rows):
        return [
            pltpu.VMEM((2 * rows, 2 * HD), jnp.bfloat16),
            pltpu.VMEM((state_rows, HD), jnp.float32),
            pltpu.VMEM((state_rows, HD), jnp.float32),
            pltpu.VMEM((BK, BK), jnp.bfloat16),
            pltpu.VMEM((2, rows, BK), jnp.float32),
            pltpu.VMEM((2, rows, BK), jnp.bfloat16),
            pltpu.VMEM((2 * y_size, tok, 2 * HD), jnp.bfloat16),
        ]

    work = 2 * y_size * rows * BK * HD * 16
    held = from_neighbours(part)
    other_query = shifted(query, "sp_2", 1)
    (closest,) = call(
        own_plane_kernel,
        [((2, rows, HD), jnp.float32)],
        (at, query, other_query, *held),
        scratch(rows),
        work // 2,
    )
    state = ()
    for k in range(1, z_size // 2 + 1):
        last = k == z_size // 2
        if k == 3:
            part, closest = lax.optimization_barrier((part, closest))
        if k == 4:
            part, early = lax.optimization_barrier((part, early))
        part = counter_shifted(part)
        held = from_neighbours(part)
        state = call(
            functools.partial(plane_kernel, k, z_size, k == 1, last),
            [((3, rows, HD), jnp.float32), ((2, rows, HD), jnp.float32)]
            if last
            else [((2, 2 * rows, HD), jnp.float32)],
            (at, query, other_query, *held) + state + ((closest,) if last else ()),
            scratch(2 * rows),
            work * 2,
        )
        state = tuple(state)
        if k == 1:
            early = state[0]
    mine, theirs = state
    return call(
        merge_kernel,
        [((tok, query.shape[1]), jnp.bfloat16)],
        (at, mine, shifted(theirs, "sp_2", 1)),
    )[0]


def chosen_slots(slots, weights, count):
    slot = lax.broadcasted_iota(jnp.int32, (slots.shape[0], count), 1)
    picked = jnp.zeros(slot.shape, jnp.float32)
    for k in range(slots.shape[1]):
        picked += jnp.where(slot == slots[:, k : k + 1], weights[:, k : k + 1], 0.0)
    return picked


def project_kernel(
    at_ref, heads_ref, w0, w1, w2, w3, stream_ref, gain_ref, slots_ref, mid_ref, normed_ref, out_ref
):
    own, count = at_ref[3], heads_ref.shape[0]
    attended = jnp.zeros(stream_ref.shape, jnp.float32)
    for k, weight in enumerate((w0, w1, w2, w3)):
        heads = heads_ref[(own + count - k) % count]
        attended += jnp.dot(heads, weight[...], preferred_element_type=jnp.float32)
    mid = (stream_ref[...].astype(jnp.float32) + attended).astype(jnp.bfloat16)
    mid_ref[...] = mid
    wide = mid.astype(jnp.float32)
    scale = lax.rsqrt(jnp.mean(wide * wide, axis=1, keepdims=True) + 1e-06)
    normed = (wide * scale * gain_ref[...]).astype(jnp.bfloat16)
    normed_ref[...] = normed
    ones = jnp.ones(slots_ref.shape, jnp.float32)
    picked = chosen_slots(slots_ref[...], ones, out_ref.shape[0]).astype(jnp.bfloat16)
    out_ref[...] = lax.dot_general(
        picked, normed, (((0,), (0,)), ((), ())), preferred_element_type=jnp.float32
    ).astype(jnp.bfloat16)


def gated(rows, gate, up):
    gate_part = jnp.dot(rows, gate, preferred_element_type=jnp.float32)
    up_part = jnp.dot(rows, up, preferred_element_type=jnp.float32)
    return (gate_part / (1.0 + jnp.exp(-gate_part)) * up_part).astype(jnp.bfloat16)


def expert_kernel(at_ref, rows_ref, gate_ref, up_ref, down_ref, out_ref):
    chunk = 256

    def part(k, _):
        here = pl.ds(pl.multiple_of(k * chunk, chunk), chunk)
        hidden = gated(rows_ref[here, :], gate_ref[...], up_ref[...])
        out_ref[here, :] = jnp.dot(
            hidden, down_ref[...], preferred_element_type=jnp.float32
        ).astype(jnp.bfloat16)
        return 0

    lax.fori_loop(0, rows_ref.shape[0] // chunk, part, 0)


def shared_kernel(at_ref, normed_ref, mid_ref, gate_ref, up_ref, down_ref, base_ref):
    hidden = gated(normed_ref[...], gate_ref[...], up_ref[...])
    base_ref[...] = mid_ref[...].astype(jnp.float32) + jnp.dot(
        hidden, down_ref[...], preferred_element_type=jnp.float32
    )


def combine_kernel(at_ref, base_ref, rows_ref, slots_ref, weights_ref, out_ref):
    picked = chosen_slots(slots_ref[...], weights_ref[...], rows_ref.shape[0])
    high = picked.astype(jnp.bfloat16)
    low = (picked - high.astype(jnp.float32)).astype(jnp.bfloat16)
    routed = jnp.dot(high, rows_ref[...], preferred_element_type=jnp.float32)
    routed += jnp.dot(low, rows_ref[...], preferred_element_type=jnp.float32)
    out_ref[...] = (base_ref[...] + routed).astype(jnp.bfloat16)


def per_device(
    query,
    key_rows,
    value_rows,
    stream,
    out_weight,
    norm_gain,
    route_ids,
    route_weights,
    expert_gate,
    expert_up,
    expert_down,
    shared_gate,
    shared_up,
    shared_down,
):
    at = jnp.stack([lax.axis_index(axis) for axis in SP_TP])
    weight_below = shifted(out_weight, "tp", 1)
    weight_above = shifted(out_weight, "tp", -1)
    weight_far = shifted(weight_below, "tp", 1)
    out_weights = (out_weight, weight_below, weight_far, weight_above)
    own_rows = stream.shape[0]
    expert_count = lax.axis_size(SP) * expert_gate.shape[0]
    capacity = 2 * own_rows * TOP_K // expert_count
    slot_count = expert_count * capacity
    flat_ids = route_ids.reshape(-1)
    membership = (flat_ids[:, None] == jnp.arange(expert_count, dtype=jnp.int32)[None, :]).astype(
        jnp.int32
    )
    before = jnp.cumsum(membership, axis=0) - membership
    slot_rank = jnp.sum(before * membership, axis=1)
    slots = (flat_ids * capacity + slot_rank).reshape(route_ids.shape)
    heads_out = attention(at, query, key_rows, value_rows)
    token_heads = lax.all_to_all(
        heads_out.reshape(-1, own_rows, heads_out.shape[1]), "tp", 0, 0, tiled=True
    )
    wide = (own_rows, D)
    mid, normed, outgoing = call(
        project_kernel,
        [(wide, jnp.bfloat16), (wide, jnp.bfloat16), ((slot_count, D), jnp.bfloat16)],
        (at, token_heads, *out_weights, stream, norm_gain.reshape(1, D), slots),
        flops=2**29,
    )
    exchange = (lax.axis_size(SP), slot_count // lax.axis_size(SP), D)
    arrived = lax.all_to_all(outgoing.reshape(exchange), SP, 0, 0, tiled=True)
    (produced,) = call(
        expert_kernel,
        [((slot_count, D), jnp.bfloat16)],
        (at, arrived.reshape(slot_count, D), expert_gate[0], expert_up[0], expert_down[0]),
        flops=2**32,
    )
    returned = lax.all_to_all(produced.reshape(exchange), SP, 0, 0, tiled=True)
    (base,) = call(
        shared_kernel,
        [(wide, jnp.float32)],
        (at, normed, mid, shared_gate, shared_up, shared_down),
        flops=2**30,
    )
    return call(
        combine_kernel,
        [(wide, jnp.bfloat16)],
        (at, base, returned.reshape(slot_count, D), slots, route_weights),
        flops=2**28,
    )[0]


def solution(mesh):
    split = Mesh(mesh.devices.reshape(8, 4, 2, mesh.shape["tp"]), ("sp_0", "sp_1", "sp_2", "tp"))
    in_specs = (
        P(SP, "tp"),
        P(SP, "tp"),
        P(SP, "tp"),
        P(SP_TP, None),
        P("tp", None),
        P(),
        P(SP_TP, None),
        P(SP_TP, None),
        P(SP, None, None),
        P(SP, None, None),
        P(SP, None, None),
        P(),
        P(),
        P(),
    )
    out_specs = P(SP_TP, None)

    return jax.shard_map(
        per_device, mesh=split, in_specs=in_specs, out_specs=out_specs, check_vma=False
    )
```
